32 devices in a mesh: sp: 8 (over z, y), tp: 4 (over x, core).
Axes of the slice: x: 2, y: 2, z: 4, core: 2. Of those that a mesh axis runs over, the one named last changes fastest.
Arguments:
- tokens: bfloat16 [4096, 2048], P(('sp', 'tp')), may hold values from -8 to 8, as said below
- w_query: bfloat16 [2048, 1024], P(None, 'tp'), may hold values from -0.125 to 0.125
- w_key: bfloat16 [2048, 1024], P(None, 'tp'), may hold values from -0.125 to 0.125
- w_value: bfloat16 [2048, 1024], P(None, 'tp'), may hold values from -0.125 to 0.125
- head_bias: float32 [16], P('tp'), may hold values from -40 to -3
- w_out: bfloat16 [1024, 2048], P('tp'), may hold values from -0.1875 to 0.1875
Outputs:
- mixed: bfloat16 [4096, 2048], P(('sp', 'tp'))
The draws below stay inside these ranges and needn't reach their ends.
Inputs may be any that keep to these rules, and one draw needn't show every extreme that they name: `tokens`: activations of order one whose mean shifts between blocks of 512 positions.
All inputs are finite; a program needn't handle non-finite values.
Results may differ from the reference program's by a relative error of at most 0.014.
Values may be sent and summed in bfloat16 or wider, within the bound.
A program may use at most 128 MiB of HBM per device.

```python
import jax
import jax.numpy as jnp
from jax import lax

D = 2048
HEADS = 16
HEAD_DIM = 64
TOK_DEV = 512
TOKENS = 4096
N_SP = 8
N_TP = 4


def draw_tokens(key, part):
    noise = jax.random.normal(jax.random.fold_in(key, 11), (TOKENS, D), jnp.float32)
    spread_level = 1.0
    direction = jax.random.normal(jax.random.fold_in(key, 12), (D,), jnp.float32)
    region_scale = jax.random.uniform(jax.random.fold_in(key, 13), (TOKENS // TOK_DEV,), jnp.float32, -1.2, 1.2)
    level = jnp.repeat(region_scale, TOK_DEV) * spread_level
    values = 0.8 * noise + level[:, None] * direction[None, :]
    return jnp.clip(values, -8.0, 8.0).astype(jnp.bfloat16)


def draw_head_bias(key, part):
    fast_count = HEADS // 2
    ranking = jax.random.permutation(jax.random.fold_in(key, 21), HEADS)
    is_fast = ranking < fast_count
    slow_value = -jnp.log(jnp.float32(TOKENS)) - 1.0 + jax.random.uniform(jax.random.fold_in(key, 22), (HEADS,), jnp.float32, -0.5, 0.5)
    fast_value = -jnp.log(jax.random.uniform(jax.random.fold_in(key, 23), (HEADS,), jnp.float32, 30.0, 100.0)) - 1.0
    return jnp.where(is_fast, fast_value, slow_value).astype(jnp.float32)


def levels(stream_key, extent, split, smallest, largest):
    gain, own = 1.0, jax.random.fold_in(stream_key, 6)
    for dim, shards_of in split:
        draws = jnp.exp(jax.random.uniform(jax.random.fold_in(own, dim), (shards_of,), jnp.float32, smallest / len(split), largest / len(split)))
        gain = gain * jnp.repeat(draws, extent[dim] // shards_of).reshape([-1 if axis == dim else 1 for axis in range(len(extent))])
    return gain


def centred(key, dims, deviation, bound, shards=(), kind=jnp.bfloat16):
    values = deviation * jax.random.normal(key, dims, jnp.float32)
    if shards:
        values = values * levels(key, dims, shards, -0.22, 0.18)
    return jnp.clip(values, -bound, bound).astype(kind)


def setup_inputs(seed: int = 0) -> dict:
    key_of = jax.random.split(jax.random.key(seed), 7)
    tokens = draw_tokens(jax.random.fold_in(key_of[6], 71), 0)
    w_query = centred(key_of[1], (D, HEADS * HEAD_DIM), D ** -0.5, 0.125, ((1, 4),))
    w_key = centred(key_of[2], (D, HEADS * HEAD_DIM), D ** -0.5, 0.125, ((1, 4),))
    w_value = centred(key_of[3], (D, HEADS * HEAD_DIM), D ** -0.5, 0.125, ((1, 4),))
    head_bias = draw_head_bias(jax.random.fold_in(key_of[6], 71), 0)
    w_out = centred(key_of[5], (HEADS * HEAD_DIM, D), (HEADS * HEAD_DIM) ** -0.5, 0.1875, ((0, 4),))
    return dict(tokens=tokens, w_query=w_query, w_key=w_key, w_value=w_value, head_bias=head_bias, w_out=w_out)


def reference(tokens, w_query, w_key, w_value, head_bias, w_out):
    query_all = jnp.dot(tokens, w_query, preferred_element_type=jnp.float32).astype(jnp.bfloat16)
    key_all = jnp.dot(tokens, w_key, preferred_element_type=jnp.float32).astype(jnp.bfloat16)
    value_all = jnp.dot(tokens, w_value, preferred_element_type=jnp.float32).astype(jnp.bfloat16)
    key_pos = jnp.arange(TOKENS, dtype=jnp.int32).reshape(N_SP, TOK_DEV)

    def by_head(head_index):
        first_col = (head_index * HEAD_DIM).astype(jnp.int32)
        query_head = lax.dynamic_slice_in_dim(query_all, first_col, HEAD_DIM, 1)
        key_head = lax.dynamic_slice_in_dim(key_all, first_col, HEAD_DIM, 1)
        value_head = lax.dynamic_slice_in_dim(value_all, first_col, HEAD_DIM, 1)
        value_segments = value_head.reshape(N_SP, TOK_DEV, HEAD_DIM).astype(jnp.float32)
        bias_value = head_bias[head_index]

        def by_block(block_index):
            first_row = (block_index * TOK_DEV).astype(jnp.int32)
            query_block = lax.dynamic_slice_in_dim(query_head, first_row, TOK_DEV, 0)
            query_pos = first_row + jnp.arange(TOK_DEV, dtype=jnp.int32)
            scores = jnp.dot(query_block, key_head.T, preferred_element_type=jnp.float32)
            scores = scores.reshape(TOK_DEV, N_SP, TOK_DEV) * (HEAD_DIM ** -0.5) + bias_value
            causal = key_pos[None] < query_pos[:, None, None]
            log_keep = jnp.where(causal, jax.nn.log_sigmoid(-scores), 0.0)
            tail = lax.cumsum(log_keep, axis=2, reverse=True) - log_keep
            weights = jnp.where(causal, jnp.exp(jax.nn.log_sigmoid(scores) + tail), 0.0).astype(jnp.bfloat16)
            segment_out = jnp.einsum('qst,std->qsd', weights.astype(jnp.float32), value_segments)
            segment_total = jnp.sum(log_keep, axis=2)
            later = lax.cumsum(segment_total, axis=1, reverse=True) - segment_total
            return jnp.sum(jnp.exp(later)[..., None] * segment_out, axis=1)

        return lax.map(by_block, jnp.arange(N_SP, dtype=jnp.int32)).reshape(TOKENS, HEAD_DIM)

    heads_out = lax.map(by_head, jnp.arange(HEADS, dtype=jnp.int32))
    attended = jnp.transpose(heads_out, (1, 0, 2)).reshape(TOKENS, HEADS * HEAD_DIM).astype(jnp.bfloat16)
    group_width = HEADS * HEAD_DIM // N_TP
    total = jnp.zeros((TOKENS, D), jnp.float32)
    for group_index in range(N_TP):
        lower = group_index * group_width
        partial_value = jnp.dot(attended[:, lower:lower + group_width], w_out[lower:lower + group_width, :],
                          preferred_element_type=jnp.float32).astype(jnp.bfloat16)
        partial_value = lax.optimization_barrier(partial_value)
        total = total + partial_value.astype(jnp.float32)
    return total.astype(jnp.bfloat16)
```

```python
import functools
import math

import jax
import jax.numpy as jnp
from jax import lax
from jax.experimental import pallas as pl
from jax.experimental.pallas import tpu as pltpu
from jax.sharding import PartitionSpec as P

MESH = pl.DeviceIdType.MESH
LOG2E = math.log2(math.e)
UNIT = 256
PARTS = 4
COLS = 512
LOOK = 4
LOG_MAX = 126.0
DEAD = -1e30


def layer_kernel(
    n_sp, n_tp, heads, bias_ref, tokens_ref, wq_ref, wk_ref, wv_ref, wo_ref, out_ref,
    tok, wqkv, wqv_t, wfull, kv_own, q_own, q_all, kv_all, packed, att, att_rows, tri,
    table, q_rhs, log_take, lose_low, weight_low, acc_ref, later_ref,
    load_sem, tok_send, tok_recv, wo_send, wo_recv, kv_send, pass_send, kv_recv, q_send, q_recv,
    back_send, back_recv,
):
    me = lax.axis_index("sp")
    col = lax.axis_index("tp")
    share_count = n_sp // heads
    device_rows = PARTS * tokens_ref.shape[1]
    width = kv_own.shape[3]
    half = width // 2
    halves = device_rows * n_tp // UNIT
    pieces = UNIT // device_rows
    visits = n_sp * halves // share_count
    blocks_per_visit = share_count // halves
    my_head = me // share_count
    my_share = lax.rem(me, share_count)
    core = lax.rem(col, 2)
    place = col // 2
    places = n_tp // 2
    sibling = place * 2 + 1 - core

    loads = [
        pltpu.make_async_copy(src, dst, load_sem.at[index])
        for index, (src, dst) in enumerate(
            [
                (tokens_ref, tok.at[col]),
                (wq_ref, wqkv.at[0]),
                (wk_ref, wqkv.at[1]),
                (wv_ref, wqkv.at[2]),
                (wo_ref, wfull.at[col]),
            ]
        )
    ]
    for copy in loads:
        copy.start()

    barrier = pltpu.get_barrier_semaphore()
    total = n_sp * n_tp
    flat = me * n_tp + col

    def greet(step, carry):
        other = lax.rem(flat + step, total)
        pl.semaphore_signal(
            barrier, inc=1, device_id=(other // n_tp, lax.rem(other, n_tp)), device_id_type=MESH
        )
        return carry

    lax.fori_loop(1, total, greet, 0)
    bias = bias_ref[my_head] * LOG2E
    row_id = lax.broadcasted_iota(jnp.int32, (UNIT, UNIT), 0)
    col_id = lax.broadcasted_iota(jnp.int32, (UNIT, UNIT), 1)
    tri[...] = jnp.where(col_id > row_id, 1.0, 0.0).astype(jnp.bfloat16)
    table[0] = jnp.full((UNIT, UNIT), bias, jnp.float32)
    table[1] = jnp.where(row_id < col_id, bias, DEAD)
    table[2] = jnp.full((UNIT, UNIT), DEAD, jnp.float32)
    for ref in (q_rhs, log_take, lose_low, weight_low, acc_ref, later_ref):
        ref[...] = jnp.zeros(ref.shape, ref.dtype)
    pl.semaphore_wait(barrier, total - 1)

    def same_core(k):
        return lax.rem(place + k, places) * 2 + core

    def arrived(ref, sem):
        pltpu.make_async_copy(ref, ref, sem).wait()

    def token_copy(kind, part):
        if kind < places:
            src, block = tokens_ref.at[part], col
            target = sibling if kind == 0 else same_core(kind)
        else:
            block = same_core(kind - places + 1)
            src, target = tok.at[block, part], sibling
        return pltpu.make_async_remote_copy(
            src_ref=src, dst_ref=tok.at[block, part],
            send_sem=tok_send.at[kind, part], recv_sem=tok_recv.at[block, part],
            device_id=(me, target), device_id_type=MESH,
        )

    def wo_copy(kind):
        if kind < places:
            src, block = wo_ref, col
            target = sibling if kind == 0 else same_core(kind)
        else:
            block = same_core(kind - places + 1)
            src, target = wfull.at[block], sibling
        return pltpu.make_async_remote_copy(
            src_ref=src, dst_ref=wfull.at[block],
            send_sem=wo_send.at[kind], recv_sem=wo_recv.at[block],
            device_id=(me, target), device_id_type=MESH,
        )

    for part in range(PARTS):
        for kind in range(places):
            token_copy(kind, part).start()
    for kind in range(1, places):
        wo_copy(kind).start()

    lane = lax.broadcasted_iota(jnp.int32, (width, width), 1)

    def turn(value):
        return pltpu.roll(value, half, 1)

    def kv_copy(step, share):
        head = lax.rem(my_head + step, heads)
        return pltpu.make_async_remote_copy(
            src_ref=kv_own.at[head, share], dst_ref=kv_all.at[me, share],
            send_sem=kv_send.at[step, share], recv_sem=kv_recv.at[me, share],
            device_id=(head * share_count + my_share, col), device_id_type=MESH,
        )

    def forward(turn_of, step, share):
        block = turn_of * share_count + my_share
        peer = my_head * share_count + lax.rem(my_share + step, share_count)
        return pltpu.make_async_remote_copy(
            src_ref=kv_all.at[block, share], dst_ref=kv_all.at[block, share],
            send_sem=pass_send.at[turn_of, step, share], recv_sem=kv_recv.at[block, share],
            device_id=(peer, col), device_id_type=MESH,
        )

    def relay(block):
        for share in range(halves):
            arrived(kv_all.at[block, share], kv_recv.at[block, share])
            for step in range(1, share_count):
                forward(block // share_count, step, share).start()

    def share_of(unit):
        place_in = lax.rem(unit, share_count)
        return jnp.where(
            lax.rem(unit // share_count, 2) == 0, place_in, share_count - 1 - place_in
        )

    def q_copy(head, share):
        unit = me * halves + share
        return pltpu.make_async_remote_copy(
            src_ref=q_own.at[head, share], dst_ref=q_all.at[unit // share_count],
            send_sem=q_send.at[head, share], recv_sem=q_recv.at[unit // share_count],
            device_id=(head * share_count + share_of(unit), col), device_id_type=MESH,
        )

    def keeps_q(head, share):
        return head * share_count + share_of(me * halves + share) == me

    def project(group):
        x = tok[pl.ds(group * pieces, pieces)].reshape(UNIT, tok.shape[3])
        across = (((1,), (1,)), ((), ()))
        scale = LOG2E * half ** (-0.5)
        kf = jnp.dot(x, wqkv[1], preferred_element_type=jnp.float32)
        vt = lax.dot_general(wqv_t[1], x, across, preferred_element_type=jnp.float32)
        qt = lax.dot_general(wqv_t[0], x, across, preferred_element_type=jnp.float32) * scale
        vt, qt = vt.astype(jnp.bfloat16), qt.astype(jnp.bfloat16)
        for pair in range(heads // 2):
            cols = slice(pair * width, (pair + 1) * width)
            top, low = kf[:width, cols], kf[width:, cols]
            kv_own[2 * pair, group, :width] = jnp.where(lane < half, top, turn(low)).astype(
                jnp.bfloat16
            )
            kv_own[2 * pair + 1, group, :width] = jnp.where(lane < half, turn(top), low).astype(
                jnp.bfloat16
            )
        for head in range(heads):
            rows = slice(head * half, (head + 1) * half)
            kv_own[head, group, width : width + half] = vt[rows, :width]
            kv_own[head, group, width + half :] = vt[rows, width:]
            q_own[head, group, :half] = qt[rows, :width]
            q_own[head, group, half:] = qt[rows, width:]
        for step in range(1, heads):
            kv_copy(step, group).start()
        kv_all[me, group] = kv_own[my_head, group]
        for step in range(1, share_count):
            forward(my_head, step, group).start()
        for head in range(heads):
            stays = keeps_q(head, group)

            @pl.when(stays)
            def _():
                q_all[(me * halves + group) // share_count] = q_own[head, group]

            @pl.when(jnp.logical_not(stays))
            def _():
                q_copy(head, group).start()

    for copy in loads:
        copy.wait()
    wqv_t[0] = wqkv[0].T
    wqv_t[1] = wqkv[2].T
    own_group = col // pieces
    early = pieces == 2
    if early:
        for part in range(PARTS):
            arrived(tok.at[sibling, part], tok_recv.at[sibling, part])
        project(own_group)
    for part in range(PARTS):
        for k in range(1, places):
            block = same_core(k)
            arrived(tok.at[block, part], tok_recv.at[block, part])
            token_copy(places + k - 1, part).start()
    for part in range(PARTS):
        if not early:
            arrived(tok.at[sibling, part], tok_recv.at[sibling, part])
        for k in range(1, places):
            block = lax.rem(place + k, places) * 2 + 1 - core
            arrived(tok.at[block, part], tok_recv.at[block, part])

    def project_next(step, carry):
        project(lax.rem(own_group + step, halves))
        return carry

    lax.fori_loop(1 if early else 0, halves, project_next, 0)

    wo_copy(0).start()

    def unit_of(visit):
        place_in = jnp.where(lax.rem(visit, 2) == 0, my_share, share_count - 1 - my_share)
        return visit * share_count + place_in

    def score(seg, kinds):
        for index in range(2):
            for side in range(2):
                rows = slice(side * width, (side + 1) * width)
                s = jnp.dot(
                    kv_all[seg, 1 - index, :width], q_rhs[side], preferred_element_type=jnp.float32
                )
                z = s + table[kinds[index], rows]
                lose = jnp.maximum(jnp.log(1.0 + jnp.exp2(jnp.minimum(z, LOG_MAX))) * LOG2E, z)
                log_take[index, rows] = z - lose
                lose_low[index, rows] = lose.astype(jnp.bfloat16)

    def weigh():
        for index in range(2):
            tail = jnp.dot(tri[...], lose_low[index], preferred_element_type=jnp.float32)
            weight_low[index] = jnp.exp2(log_take[index] - tail).astype(jnp.bfloat16)
            later_ref[index + 1 : index + 2] = tail[0:1] + lose_low[index, 0:1].astype(jnp.float32)

    def gather(visit, seg):
        first = seg == unit_of(visit) // halves
        acc = jnp.where(first, 0.0, acc_ref[...])
        later = jnp.where(first, 0.0, later_ref[0:1])
        for index in range(2):
            values = kv_all[seg, 1 - index, width:]
            values = jnp.concatenate([values[:half], values[half:]], axis=1)
            out = jnp.dot(values, weight_low[index], preferred_element_type=jnp.float32)
            acc = acc + jnp.exp2(-later) * out
            later = later + later_ref[index + 1 : index + 2]
        acc_ref[...] = acc
        later_ref[0:1] = later

    def is_here(visit, index):
        unit = unit_of(visit)
        owner = lax.rem(unit, halves) * pieces + index
        return jnp.logical_and(unit // halves == me, owner == col)

    def back(visit, index):
        unit = unit_of(visit)
        owner = lax.rem(unit, halves) * pieces + index
        slot = col * heads + my_head
        return pltpu.make_async_remote_copy(
            src_ref=packed.at[visit, index], dst_ref=att.at[slot],
            send_sem=back_send.at[visit, index], recv_sem=back_recv.at[slot],
            device_id=(unit // halves, owner), device_id_type=MESH,
        )

    def send_home(visit):
        for index in range(pieces):
            piece = acc_ref[:, index * device_rows : (index + 1) * device_rows]
            packed[visit, index] = piece.astype(jnp.bfloat16)
            here = is_here(visit, index)

            @pl.when(here)
            def _():
                att[col * heads + my_head] = packed[visit, index]

            @pl.when(jnp.logical_not(here))
            def _():
                back(visit, index).start()

    def relayed(block):
        return jnp.logical_and(lax.rem(block, share_count) == my_share, block != me)

    for block in range(min(LOOK, n_sp)):

        @pl.when(relayed(block))
        def _():
            relay(block)

    def visit_blocks(visit, carry):
        for offset in range(blocks_per_visit):
            block = visit * blocks_per_visit + offset
            ahead = block + LOOK

            @pl.when(jnp.logical_and(ahead < n_sp, relayed(ahead)))
            def _():
                relay(ahead)

            @pl.when(lax.rem(block, share_count) != my_share)
            def _():
                for share in range(halves):
                    arrived(kv_all.at[block, share], kv_recv.at[block, share])

        unit = unit_of(visit)
        block, side = unit // halves, lax.rem(unit, halves)
        @pl.when(block != me)
        def _():
            arrived(q_all.at[visit], q_recv.at[visit])

        @pl.when(visit == visits - 1)
        def _():
            for k in range(1, places):
                arrived(wfull.at[same_core(k)], wo_recv.at[same_core(k)])
                wo_copy(places + k - 1).start()

        pair = q_all[visit]
        queries = jnp.concatenate([pair[:half], pair[half:]], axis=1)
        q_rhs[0, :half] = queries
        q_rhs[1, half:] = queries

        def step_segment(step, state):
            last_visit, last_seg, real = state
            seg = block - step
            own = step == 0
            kinds = (jnp.where(own, 2 - side, 0), jnp.where(own, 1 - side, 0))
            weigh()
            score(seg, kinds)
            gather(last_visit, last_seg)

            @pl.when(jnp.logical_and(last_seg == 0, real == 1))
            def _():
                send_home(last_visit)

            return visit, seg, jnp.int32(1)

        return lax.fori_loop(0, block + 1, step_segment, carry)

    none = jnp.int32(0)
    last_visit, last_seg, _ = lax.fori_loop(0, visits, visit_blocks, (none, none, none))
    weigh()
    gather(last_visit, last_seg)
    send_home(last_visit)

    my_unit = me * halves + col * device_rows // UNIT
    for source_col in range(n_tp):
        for head in range(heads):
            slot = source_col * heads + head
            source = head * share_count + share_of(my_unit)

            @pl.when(jnp.logical_not(jnp.logical_and(source == me, source_col == col)))
            def _():
                arrived(att.at[slot], back_recv.at[slot])

    att_rows[...] = att[...].reshape(att_rows.shape[1], device_rows).T
    arrived(wfull.at[sibling], wo_recv.at[sibling])
    for k in range(1, places):
        block = lax.rem(place + k, places) * 2 + 1 - core
        arrived(wfull.at[block], wo_recv.at[block])
    for first in range(0, out_ref.shape[1], COLS):
        w = wfull[:, :, first : first + COLS].reshape(att_rows.shape[1], COLS)
        out_ref[:, first : first + COLS] = jnp.dot(
            att_rows[...], w, preferred_element_type=jnp.float32
        ).astype(jnp.bfloat16)

    for kind in range(2 * places - 1):
        wo_copy(kind).wait_send()
        for part in range(PARTS):
            token_copy(kind, part).wait_send()
    for share in range(halves):
        for head in range(heads):

            @pl.when(jnp.logical_not(keeps_q(head, share)))
            def _():
                q_copy(head, share).wait_send()

        for step in range(1, heads):
            kv_copy(step, share).wait_send()
        for turn_of in range(heads):
            for step in range(1, share_count):
                forward(turn_of, step, share).wait_send()

    def drain(visit, carry):
        for index in range(pieces):

            @pl.when(jnp.logical_not(is_here(visit, index)))
            def _():
                back(visit, index).wait_send()

        return carry

    lax.fori_loop(0, visits, drain, 0)


def shards(tokens, w_query, w_key, w_value, head_bias, w_out):
    model, local_width = w_query.shape
    heads = head_bias.shape[0]
    half = local_width // heads
    width = 2 * half
    n_sp = lax.axis_size("sp")
    n_tp = lax.axis_size("tp")
    device_rows = tokens.shape[0]
    share_count = n_sp // heads
    halves = device_rows * n_tp // UNIT
    pieces = UNIT // device_rows
    visits = n_sp * halves // share_count
    slots = n_tp * heads
    out_width = w_out.shape[1]
    places = n_tp // 2
    kinds = 2 * places - 1

    smem = pl.BlockSpec(memory_space=pltpu.SMEM)
    anywhere = pl.BlockSpec(memory_space=pl.ANY)
    dma = pltpu.SemaphoreType.DMA

    def vmem(*shape):
        return pltpu.VMEM(shape, jnp.bfloat16)

    def wide(*shape):
        return pltpu.VMEM(shape, jnp.float32)

    return pl.pallas_call(
        functools.partial(layer_kernel, n_sp, n_tp, heads),
        out_shape=jax.ShapeDtypeStruct((device_rows, out_width), jnp.bfloat16),
        in_specs=[smem] + [anywhere] * 5,
        out_specs=pl.BlockSpec(memory_space=pltpu.VMEM),
        scratch_shapes=[
            vmem(n_tp, PARTS, device_rows // PARTS, model),
            vmem(3, model, local_width),
            vmem(2, local_width, model),
            vmem(n_tp, local_width, out_width),
            vmem(heads, halves, UNIT, width),
            vmem(heads, halves, UNIT // 2, width),
            vmem(visits, UNIT // 2, width),
            vmem(n_sp, halves, UNIT, width),
            vmem(visits, pieces, half, device_rows),
            vmem(slots, half, device_rows),
            vmem(device_rows, n_tp * local_width),
            vmem(UNIT, UNIT),
            wide(3, UNIT, UNIT),
            vmem(2, width, UNIT),
            wide(2, UNIT, UNIT),
            vmem(2, UNIT, UNIT),
            vmem(2, UNIT, UNIT),
            wide(half, UNIT),
            wide(8, UNIT),
            dma((5,)),
            dma((kinds, PARTS)),
            dma((n_tp, PARTS)),
            dma((kinds,)),
            dma((n_tp,)),
            dma((heads, halves)),
            dma((heads, share_count, halves)),
            dma((n_sp, halves)),
            dma((heads, halves)),
            dma((visits,)),
            dma((visits, pieces)),
            dma((slots,)),
        ],
        compiler_params=pltpu.CompilerParams(
            collective_id=0, has_side_effects=True, vmem_limit_bytes=60 * 2**20
        ),
        name="layer",
    )(
        head_bias,
        tokens.reshape(PARTS, device_rows // PARTS, model),
        w_query, w_key, w_value, w_out,
    )


def solution(mesh):
    placed = (
        P(("sp", "tp"), None),
        P(None, "tp"),
        P(None, "tp"),
        P(None, "tp"),
        P("tp"),
        P("tp", None),
    )
    return jax.shard_map(
        shards, mesh=mesh, in_specs=placed, out_specs=P(("sp", "tp"), None), check_vma=False
    )
```

```python
import functools
import math

import jax
import jax.numpy as jnp
from jax import lax
from jax.experimental import pallas as pl
from jax.experimental.pallas import tpu as pltpu
from jax.sharding import PartitionSpec as P

MESH = pl.DeviceIdType.MESH
LOG2E = math.log2(math.e)
UNIT = 256
PARTS = 4
COLS = 512
WO_PART = 8
WO_TURN = 0
FAR_RELAY = 2
LAST_RELAY = 4
LOG_MAX = 126.0
DEAD = -1e30


def layer_kernel(
    n_sp, n_tp, heads, bias_ref, tokens_ref, wq_ref, wk_ref, wv_ref, wo_ref, out_ref,
    tok, wqkv, wqv_t, wfull, kv_own, q_own, q_all, kv_all, packed, att, att_rows, tri,
    table, q_rhs, log_take, lose_low, weight_low, acc_ref, later_ref, done_ref,
    load_sem, tok_send, tok_recv, wo_send, wo_recv, kv_send, pass_send, kv_recv, q_send, q_recv,
    back_send, back_recv,
):
    me = lax.axis_index("sp")
    col = lax.axis_index("tp")
    share_count = n_sp // heads
    device_rows = PARTS * tokens_ref.shape[1]
    width = kv_own.shape[3]
    half = width // 2
    local_width = heads * half
    halves = device_rows * n_tp // UNIT
    pieces = UNIT // device_rows
    visits = n_sp * halves // share_count
    blocks_per_visit = share_count // halves
    my_head = me // share_count
    my_share = lax.rem(me, share_count)
    own_group = col // pieces
    early = pieces == 2 and halves == 2
    core = lax.rem(col, 2)
    place = col // 2
    places = n_tp // 2
    sibling = place * 2 + 1 - core

    loads = [
        pltpu.make_async_copy(src, dst, load_sem.at[index])
        for index, (src, dst) in enumerate(
            [
                (tokens_ref, tok.at[col]),
                (wq_ref, wqkv.at[0]),
                (wk_ref, wqkv.at[1]),
                (wv_ref, wqkv.at[2]),
                (wo_ref, wfull.at[col]),
            ]
        )
    ]
    for copy in loads:
        copy.start()

    barrier = pltpu.get_barrier_semaphore()
    total = n_sp * n_tp
    flat = me * n_tp + col

    def greet(step, carry):
        other = lax.rem(flat + step, total)
        pl.semaphore_signal(
            barrier, inc=1, device_id=(other // n_tp, lax.rem(other, n_tp)), device_id_type=MESH
        )
        return carry

    lax.fori_loop(1, total, greet, 0)
    bias = bias_ref[my_head] * LOG2E
    row_id = lax.broadcasted_iota(jnp.int32, (UNIT, UNIT), 0)
    col_id = lax.broadcasted_iota(jnp.int32, (UNIT, UNIT), 1)
    tri[...] = jnp.where(col_id > row_id, 1.0, 0.0).astype(jnp.bfloat16)
    table[0] = jnp.full((UNIT, UNIT), bias, jnp.float32)
    table[1] = jnp.where(row_id < col_id, bias, DEAD)
    table[2] = jnp.full((UNIT, UNIT), DEAD, jnp.float32)
    for ref in (q_rhs, log_take, lose_low, weight_low, acc_ref, later_ref, done_ref):
        ref[...] = jnp.zeros(ref.shape, ref.dtype)
    pl.semaphore_wait(barrier, total - 1)

    def same_core(k):
        return lax.rem(place + k, places) * 2 + core

    def arrived(ref, sem):
        pltpu.make_async_copy(ref, ref, sem).wait()

    def token_copy(kind, part):
        if kind < places:
            src, block = tokens_ref.at[part], col
            target = sibling if kind == 0 else same_core(kind)
        else:
            block = same_core(kind - places + 1)
            src, target = tok.at[block, part], sibling
        return pltpu.make_async_remote_copy(
            src_ref=src, dst_ref=tok.at[block, part],
            send_sem=tok_send.at[kind, part], recv_sem=tok_recv.at[block, part],
            device_id=(me, target), device_id_type=MESH,
        )

    shared = local_width // WO_PART
    odd = lax.rem(me, 2)

    def band_of(which):
        if which == 2:
            return pl.ds(2 * shared, local_width - 2 * shared)
        return pl.ds(pl.multiple_of((odd if which == 0 else 1 - odd) * shared, 16), shared)

    def to_band(which):
        if which == 2:
            return 2
        return odd if which == 0 else 1 - odd

    def wo_send_copy(block, which, target, slot):
        rows = band_of(which)
        return pltpu.make_async_remote_copy(
            src_ref=wfull.at[block, rows], dst_ref=wfull.at[block, rows],
            send_sem=wo_send.at[slot, which], recv_sem=wo_recv.at[block, to_band(which)],
            device_id=target, device_id_type=MESH,
        )

    def wo_arrived(block, which):
        ref = wfull.at[block, band_of(which)]
        arrived(ref, wo_recv.at[block, to_band(which)])

    def wo_across(k, which):
        return wo_send_copy(col, which, (me, same_core(k)), k)

    def wo_aside(k, which):
        block = col if k == 0 else same_core(k)
        return wo_send_copy(block, which, (me, sibling), 0 if k == 0 else places + k - 1)

    def wo_partner(k):
        return wo_send_copy(same_core(k), 0, (me + 1 - 2 * odd, col), 2 * places - 2 + k)

    for part in range(PARTS):
        for kind in range(places):
            token_copy(kind, part).start()

    lane = lax.broadcasted_iota(jnp.int32, (width, width), 1)

    def turn(value):
        return pltpu.roll(value, half, 1)

    def head_at(step):
        base = lax.rem(my_head + step // 2 * 2, heads)
        return base + lax.rem(step, 2) * (1 - 2 * lax.rem(base, 2))

    def kv_copy(step, share):
        head = head_at(step)
        return pltpu.make_async_remote_copy(
            src_ref=kv_own.at[head, share], dst_ref=kv_all.at[me, share],
            send_sem=kv_send.at[step, share], recv_sem=kv_recv.at[me, share],
            device_id=(head * share_count + my_share, col), device_id_type=MESH,
        )

    def forward(turn_of, step, share):
        block = turn_of * share_count + my_share
        peer = my_head * share_count + lax.rem(my_share + step, share_count)
        return pltpu.make_async_remote_copy(
            src_ref=kv_all.at[block, share], dst_ref=kv_all.at[block, share],
            send_sem=pass_send.at[turn_of, step, share], recv_sem=kv_recv.at[block, share],
            device_id=(peer, col), device_id_type=MESH,
        )

    def relay_one(block, share):
        arrived(kv_all.at[block, share], kv_recv.at[block, share])
        for step in range(1, share_count):
            forward(block // share_count, step, share).start()

    def relay(block):
        if early:
            relay_one(block, 1 - own_group)
        else:
            for share in range(halves):
                relay_one(block, share)

    def share_of(unit):
        place_in = lax.rem(unit, share_count)
        return jnp.where(
            lax.rem(unit // share_count, 2) == 0, place_in, share_count - 1 - place_in
        )

    def q_copy(step, share):
        head = head_at(step)
        unit = me * halves + share
        return pltpu.make_async_remote_copy(
            src_ref=q_own.at[head, share], dst_ref=q_all.at[unit // share_count],
            send_sem=q_send.at[step, share], recv_sem=q_recv.at[unit // share_count],
            device_id=(head * share_count + share_of(unit), col), device_id_type=MESH,
        )

    def keeps_q(share):
        return share_of(me * halves + share) == my_share

    def project(group):
        x = tok[pl.ds(group * pieces, pieces)].reshape(UNIT, tok.shape[3])
        across = (((1,), (1,)), ((), ()))
        scale = LOG2E * half ** (-0.5)
        kf = jnp.dot(x, wqkv[1], preferred_element_type=jnp.float32)
        vt = lax.dot_general(wqv_t[1], x, across, preferred_element_type=jnp.float32)
        qt = lax.dot_general(wqv_t[0], x, across, preferred_element_type=jnp.float32) * scale
        vt, qt = vt.astype(jnp.bfloat16), qt.astype(jnp.bfloat16)
        for pair in range(heads // 2):
            cols = slice(pair * width, (pair + 1) * width)
            top, low = kf[:width, cols], kf[width:, cols]
            kv_own[2 * pair, group, :width] = jnp.where(lane < half, top, turn(low)).astype(
                jnp.bfloat16
            )
            kv_own[2 * pair + 1, group, :width] = jnp.where(lane < half, turn(top), low).astype(
                jnp.bfloat16
            )
        for head in range(heads):
            rows = slice(head * half, (head + 1) * half)
            kv_own[head, group, width : width + half] = vt[rows, :width]
            kv_own[head, group, width + half :] = vt[rows, width:]
            q_own[head, group, :half] = qt[rows, :width]
            q_own[head, group, half:] = qt[rows, width:]
        kv_all[me, group] = kv_own[my_head, group]
        for step in range(1, share_count):
            forward(my_head, step, group).start()
        for first in range(0, heads, 2):
            for step in range(max(first, 1), first + 2):
                kv_copy(step, group).start()
            for step in range(first, first + 2):
                if step > 0:
                    q_copy(step, group).start()
                else:
                    stays = keeps_q(group)

                    @pl.when(stays)
                    def _():
                        q_all[(me * halves + group) // share_count] = q_own[my_head, group]

                    @pl.when(jnp.logical_not(stays))
                    def _():
                        q_copy(0, group).start()

    for copy in loads:
        copy.wait()
    for which in (0, 2):
        for k in range(1, places):
            wo_across(k, which).start()
    wqv_t[0] = wqkv[0].T
    wqv_t[1] = wqkv[2].T
    if early:
        for part in range(PARTS):
            arrived(tok.at[sibling, part], tok_recv.at[sibling, part])
        project(own_group)
    for part in range(PARTS):
        if early and part == PARTS - 1:
            for turn_of in range(heads):

                @pl.when(turn_of != my_head)
                def _():
                    relay_one(turn_of * share_count + my_share, own_group)

        for k in range(1, places):
            block = same_core(k)
            arrived(tok.at[block, part], tok_recv.at[block, part])
            token_copy(places + k - 1, part).start()
    for part in range(PARTS):
        if not early:
            arrived(tok.at[sibling, part], tok_recv.at[sibling, part])
        for k in range(1, places):
            block = lax.rem(place + k, places) * 2 + 1 - core
            arrived(tok.at[block, part], tok_recv.at[block, part])

    def project_next(step, carry):
        project(lax.rem(own_group + step, halves))
        return carry

    lax.fori_loop(1 if early else 0, halves, project_next, 0)

    for which in range(3):
        wo_aside(0, which).start()

    def unit_of(visit):
        place_in = jnp.where(lax.rem(visit, 2) == 0, my_share, share_count - 1 - my_share)
        return visit * share_count + place_in

    def score(visit, seg, kinds):
        for index in range(2):
            for side in range(2):
                rows = slice(side * width, (side + 1) * width)
                s = jnp.dot(
                    kv_all[seg, 1 - index, :width], q_rhs[visit, side], preferred_element_type=jnp.float32
                )
                z = jnp.minimum(s + table[kinds[index], rows], LOG_MAX)
                lose = jnp.log(1.0 + jnp.exp2(z)) * LOG2E
                log_take[index, rows] = z - lose
                lose_low[index, rows] = lose.astype(jnp.bfloat16)

    def weigh():
        for index in range(2):
            tail = jnp.dot(tri[...], lose_low[index], preferred_element_type=jnp.float32)
            weight_low[index] = jnp.exp2(log_take[index] - tail).astype(jnp.bfloat16)
            later_ref[index : index + 1] = tail[0:1] + lose_low[index, 0:1].astype(jnp.float32)

    def gather(visit, seg):
        first = seg == unit_of(visit) // halves
        acc = jnp.where(first, 0.0, acc_ref[visit])
        later = jnp.where(first, 0.0, done_ref[visit, 0:1])
        for index in range(2):
            values = kv_all[seg, 1 - index, width:]
            values = jnp.concatenate([values[:half], values[half:]], axis=1)
            out = jnp.dot(values, weight_low[index], preferred_element_type=jnp.float32)
            acc = acc + jnp.exp2(-later) * out
            later = later + later_ref[index : index + 1]
        acc_ref[visit] = acc
        done_ref[visit, 0:1] = later

    def is_here(visit, index):
        unit = unit_of(visit)
        owner = lax.rem(unit, halves) * pieces + index
        return jnp.logical_and(unit // halves == me, owner == col)

    def back(visit, index):
        unit = unit_of(visit)
        owner = lax.rem(unit, halves) * pieces + index
        slot = col * heads + my_head
        return pltpu.make_async_remote_copy(
            src_ref=packed.at[visit, index], dst_ref=att.at[slot],
            send_sem=back_send.at[visit, index], recv_sem=back_recv.at[slot],
            device_id=(unit // halves, owner), device_id_type=MESH,
        )

    def send_home(visit):
        for index in range(pieces):
            piece = acc_ref[visit, :, index * device_rows : (index + 1) * device_rows]
            packed[visit, index] = piece.astype(jnp.bfloat16)
            here = is_here(visit, index)

            @pl.when(here)
            def _():
                att[col * heads + my_head] = packed[visit, index]

            @pl.when(jnp.logical_not(here))
            def _():
                back(visit, index).start()

    def relayed(block):
        return jnp.logical_and(lax.rem(block, share_count) == my_share, block != me)

    halved = blocks_per_visit == 1 and n_sp % 4 == 0
    near, quarter = n_sp // 2, n_sp // 4
    upper = my_head >= heads // 2

    def pick(low, high):
        return jnp.where(upper, high, low) if halved else low

    swept = lax.rem(my_head, 2) == 1

    def block_at(turn_count):
        distant = turn_count - near - quarter
        far = pick(turn_count, jnp.where(distant < 0, n_sp - 1 - turn_count, distant))
        close = jnp.where(swept, near - 1 - turn_count, turn_count) + pick(0, near)
        return jnp.where(turn_count < near, close, far)

    def relay_from(first, last):
        def one(index, carry):
            block = block_at(index)

            @pl.when(relayed(block))
            def _():
                relay(block)

            return carry

        lax.fori_loop(first, last, one, 0)

    def expect(block):
        @pl.when(lax.rem(block, share_count) != my_share)
        def _():
            for share in range(halves):
                arrived(kv_all.at[block, share], kv_recv.at[block, share])

    def expect_queries(visit):
        @pl.when(unit_of(visit) // halves != me)
        def _():
            arrived(q_all.at[visit], q_recv.at[visit])

        pair = q_all[visit]
        queries = jnp.concatenate([pair[:half], pair[half:]], axis=1)
        q_rhs[visit, 0, :half] = queries
        q_rhs[visit, 1, half:] = queries

    turns = n_sp + near if halved else visits
    relay_from(0, near if halved else n_sp)

    def take_turn(turn_count, carry):
        if halved:

            @pl.when(turn_count == FAR_RELAY)
            def _():
                relay_from(near, near + quarter)

            @pl.when(turn_count == LAST_RELAY)
            def _():
                relay_from(near + quarter, n_sp)

            @pl.when(turn_count < n_sp)
            def _():
                expect(block_at(turn_count))

            distant = turn_count - near - quarter
            home = turn_count < near
            block = block_at(turn_count)
            late = jnp.logical_and(distant >= 0, distant < near)
            asks = jnp.logical_or(home, pick(turn_count < n_sp, late))
            asked = jnp.where(home, block, pick(turn_count, distant))

            @pl.when(asks)
            def _():
                expect_queries(asked)

            along = jnp.where(home, swept, jnp.logical_and(upper, jnp.logical_not(late)))
            rest = jnp.where(distant < 0, n_sp - 1 - turn_count, turns - 1 - turn_count)
            far_seg = jnp.where(along, rest, asked)
            seg = jnp.where(home, block, far_seg)
            visit = jnp.where(home, block, jnp.where(along, near, asked))
            far_count = pick(
                jnp.where(turn_count < n_sp, turn_count + 1, 0),
                jnp.where(late, distant + 1, near),
            )
            count = jnp.where(home, turn_count + 1, far_count)
            forth = jnp.where(along, 1, 0)
            wo_first, wo_last = near + WO_TURN, pick(n_sp - 1, n_sp + 2)
        else:
            for offset in range(blocks_per_visit):
                expect(turn_count * blocks_per_visit + offset)
            expect_queries(turn_count)
            visit, seg = turn_count, unit_of(turn_count) // halves
            count, forth = seg + 1, 0
            wo_first, wo_last = visits // 2, visits - 1

        @pl.when(turn_count == wo_first)
        def _():
            for k in range(1, places):
                wo_arrived(same_core(k), 0)
                wo_partner(k).start()
                wo_aside(k, 0).start()

        @pl.when(turn_count == wo_last)
        def _():
            for k in range(1, places):
                for which in (2, 1):
                    wo_arrived(same_core(k), which)
                    wo_aside(k, which).start()

        def step_segment(step, state):
            last_visit, last_seg, real = state
            now = visit + forth * step
            part = seg - (1 - forth) * step
            unit = unit_of(now)
            own, side = part == unit // halves, lax.rem(unit, halves)
            kinds = (jnp.where(own, 2 - side, 0), jnp.where(own, 1 - side, 0))
            weigh()
            score(now, part, kinds)
            gather(last_visit, last_seg)

            @pl.when(jnp.logical_and(last_seg == 0, real == 1))
            def _():
                send_home(last_visit)

            return now, part, jnp.int32(1)

        return lax.fori_loop(0, count, step_segment, carry)

    start = jnp.int32(0) + (block_at(0) if halved else 0)
    last_visit, last_seg, _ = lax.fori_loop(0, turns, take_turn, (start, start, jnp.int32(0)))
    weigh()
    gather(last_visit, last_seg)
    send_home(last_visit)

    my_unit = me * halves + col * device_rows // UNIT
    for source_col in range(n_tp):
        for head in range(heads):
            slot = source_col * heads + head
            source = head * share_count + share_of(my_unit)

            @pl.when(jnp.logical_not(jnp.logical_and(source == me, source_col == col)))
            def _():
                arrived(att.at[slot], back_recv.at[slot])

    att_rows[...] = att[...].reshape(att_rows.shape[1], device_rows).T
    for k in range(places):
        for which in range(3):
            wo_arrived(lax.rem(place + k, places) * 2 + 1 - core, which)
    for first in range(0, out_ref.shape[1], COLS):
        w = wfull[:, :, first : first + COLS].reshape(att_rows.shape[1], COLS)
        out_ref[:, first : first + COLS] = jnp.dot(
            att_rows[...], w, preferred_element_type=jnp.float32
        ).astype(jnp.bfloat16)

    for k in range(places):
        for which in range(3):
            wo_aside(k, which).wait_send()
    for k in range(1, places):
        wo_partner(k).wait_send()
        for which in (0, 2):
            wo_across(k, which).wait_send()
    for kind in range(2 * places - 1):
        for part in range(PARTS):
            token_copy(kind, part).wait_send()
    for share in range(halves):
        @pl.when(jnp.logical_not(keeps_q(share)))
        def _():
            q_copy(0, share).wait_send()

        for step in range(1, heads):
            q_copy(step, share).wait_send()
        for step in range(1, heads):
            kv_copy(step, share).wait_send()
        for turn_of in range(heads):
            for step in range(1, share_count):
                forward(turn_of, step, share).wait_send()

    def drain(visit, carry):
        for index in range(pieces):

            @pl.when(jnp.logical_not(is_here(visit, index)))
            def _():
                back(visit, index).wait_send()

        return carry

    lax.fori_loop(0, visits, drain, 0)


def shards(tokens, w_query, w_key, w_value, head_bias, w_out):
    model, local_width = w_query.shape
    heads = head_bias.shape[0]
    half = local_width // heads
    width = 2 * half
    n_sp = lax.axis_size("sp")
    n_tp = lax.axis_size("tp")
    device_rows = tokens.shape[0]
    share_count = n_sp // heads
    halves = device_rows * n_tp // UNIT
    pieces = UNIT // device_rows
    visits = n_sp * halves // share_count
    slots = n_tp * heads
    out_width = w_out.shape[1]
    places = n_tp // 2
    kinds = 2 * places - 1

    smem = pl.BlockSpec(memory_space=pltpu.SMEM)
    anywhere = pl.BlockSpec(memory_space=pl.ANY)
    dma = pltpu.SemaphoreType.DMA

    def vmem(*shape):
        return pltpu.VMEM(shape, jnp.bfloat16)

    def wide(*shape):
        return pltpu.VMEM(shape, jnp.float32)

    return pl.pallas_call(
        functools.partial(layer_kernel, n_sp, n_tp, heads),
        out_shape=jax.ShapeDtypeStruct((device_rows, out_width), jnp.bfloat16),
        in_specs=[smem] + [anywhere] * 5,
        out_specs=pl.BlockSpec(memory_space=pltpu.VMEM),
        scratch_shapes=[
            vmem(n_tp, PARTS, device_rows // PARTS, model),
            vmem(3, model, local_width),
            vmem(2, local_width, model),
            vmem(n_tp, local_width, out_width),
            vmem(heads, halves, UNIT, width),
            vmem(heads, halves, UNIT // 2, width),
            vmem(visits, UNIT // 2, width),
            vmem(n_sp, halves, UNIT, width),
            vmem(visits, pieces, half, device_rows),
            vmem(slots, half, device_rows),
            vmem(device_rows, n_tp * local_width),
            vmem(UNIT, UNIT),
            wide(3, UNIT, UNIT),
            vmem(visits, 2, width, UNIT),
            wide(2, UNIT, UNIT),
            vmem(2, UNIT, UNIT),
            vmem(2, UNIT, UNIT),
            wide(visits, half, UNIT),
            wide(8, UNIT),
            wide(visits, 8, UNIT),
            dma((5,)),
            dma((kinds, PARTS)),
            dma((n_tp, PARTS)),
            dma((3 * places - 2, 3)),
            dma((n_tp, 3)),
            dma((heads, halves)),
            dma((heads, share_count, halves)),
            dma((n_sp, halves)),
            dma((heads, halves)),
            dma((visits,)),
            dma((visits, pieces)),
            dma((slots,)),
        ],
        compiler_params=pltpu.CompilerParams(
            collective_id=0, has_side_effects=True, vmem_limit_bytes=53 * 2**20
        ),
        name="layer",
    )(
        head_bias,
        tokens.reshape(PARTS, device_rows // PARTS, model),
        w_query, w_key, w_value, w_out,
    )


def solution(mesh):
    placed = (
        P(("sp", "tp"), None),
        P(None, "tp"),
        P(None, "tp"),
        P(None, "tp"),
        P("tp"),
        P("tp", None),
    )
    return jax.shard_map(
        shards, mesh=mesh, in_specs=placed, out_specs=P(("sp", "tp"), None), check_vma=False
    )
```

```python
import functools
import math

import jax
import jax.numpy as jnp
from jax import lax
from jax.experimental import pallas as pl
from jax.experimental.pallas import tpu as pltpu
from jax.sharding import PartitionSpec as P

MESH = pl.DeviceIdType.MESH
LOG2E = math.log2(math.e)
UNIT = 256
PARTS = 4
COLS = 512
WO_PART = 8
WO_TURN = 0
FAR_RELAY = 2
LAST_RELAY = 3
LOG_MAX = 126.0
DEAD = -1e30


def layer_kernel(
    n_sp, n_tp, heads, bias_ref, tokens_ref, wq_ref, wk_ref, wv_ref, wo_ref, out_ref,
    tok, wqkv, wqv_t, wfull, kv_own, q_own, q_all, kv_all, packed, att, att_rows, tri,
    table, q_rhs, log_take, lose_low, weight_low, acc_ref, later_ref, done_ref,
    load_sem, tok_send, tok_recv, wo_send, wo_recv, kv_send, pass_send, kv_recv, q_send, q_recv,
    back_send, back_recv,
):
    me = lax.axis_index("sp")
    col = lax.axis_index("tp")
    share_count = n_sp // heads
    device_rows = PARTS * tokens_ref.shape[1]
    width = kv_own.shape[4]
    half = width // 2
    local_width = heads * half
    halves = device_rows * n_tp // UNIT
    pieces = UNIT // device_rows
    visits = n_sp * halves // share_count
    blocks_per_visit = share_count // halves
    my_head = me // share_count
    my_share = lax.rem(me, share_count)
    own_group = col // pieces
    early = pieces == 2 and halves == 2
    core = lax.rem(col, 2)
    place = col // 2
    places = n_tp // 2
    sibling = place * 2 + 1 - core

    loads = [
        pltpu.make_async_copy(src, dst, load_sem.at[index])
        for index, (src, dst) in enumerate(
            [
                (tokens_ref, tok.at[col]),
                (wq_ref, wqkv.at[0]),
                (wk_ref, wqkv.at[1]),
                (wv_ref, wqkv.at[2]),
                (wo_ref, wfull.at[col]),
            ]
        )
    ]
    for copy in loads:
        copy.start()

    barrier = pltpu.get_barrier_semaphore()
    total = n_sp * n_tp
    flat = me * n_tp + col

    def greet(step, carry):
        other = lax.rem(flat + step, total)
        pl.semaphore_signal(
            barrier, inc=1, device_id=(other // n_tp, lax.rem(other, n_tp)), device_id_type=MESH
        )
        return carry

    lax.fori_loop(1, total, greet, 0)
    bias = bias_ref[my_head] * LOG2E
    row_id = lax.broadcasted_iota(jnp.int32, (UNIT, UNIT), 0)
    col_id = lax.broadcasted_iota(jnp.int32, (UNIT, UNIT), 1)
    run = device_rows // 2
    run_bits = run.bit_length() - 1

    def position(index):
        inner = index & (width - 1)
        block = lax.shift_right_logical(inner, run_bits)
        side = lax.shift_right_logical(index, width.bit_length() - 1)
        return block * device_rows + side * run + (inner & (run - 1))

    row_id, col_id = position(row_id), position(col_id)
    tri[...] = jnp.where(col_id > row_id, 1.0, 0.0).astype(jnp.bfloat16)
    table[0] = jnp.full((UNIT, UNIT), bias, jnp.float32)
    table[1] = jnp.where(row_id < col_id, bias, DEAD)
    table[2] = jnp.full((UNIT, UNIT), DEAD, jnp.float32)
    for ref in (q_rhs, log_take, lose_low, weight_low, acc_ref, later_ref, done_ref):
        ref[...] = jnp.zeros(ref.shape, ref.dtype)
    pl.semaphore_wait(barrier, total - 1)

    def same_core(k):
        return lax.rem(place + k, places) * 2 + core

    def arrived(ref, sem):
        pltpu.make_async_copy(ref, ref, sem).wait()

    def token_copy(kind, part):
        if kind < places:
            src, block = tokens_ref.at[part], col
            target = sibling if kind == 0 else same_core(kind)
        else:
            block = same_core(kind - places + 1)
            src, target = tok.at[block, part], sibling
        return pltpu.make_async_remote_copy(
            src_ref=src, dst_ref=tok.at[block, part],
            send_sem=tok_send.at[kind, part], recv_sem=tok_recv.at[block, part],
            device_id=(me, target), device_id_type=MESH,
        )

    shared = local_width // WO_PART
    odd = lax.rem(me, 2)

    def band_of(which):
        if which == 2:
            return pl.ds(2 * shared, local_width - 2 * shared)
        return pl.ds(pl.multiple_of((odd if which == 0 else 1 - odd) * shared, 16), shared)

    def to_band(which):
        if which == 2:
            return 2
        return odd if which == 0 else 1 - odd

    def wo_send_copy(block, which, target, slot):
        rows = band_of(which)
        return pltpu.make_async_remote_copy(
            src_ref=wfull.at[block, rows], dst_ref=wfull.at[block, rows],
            send_sem=wo_send.at[slot, which], recv_sem=wo_recv.at[block, to_band(which)],
            device_id=target, device_id_type=MESH,
        )

    def wo_arrived(block, which):
        ref = wfull.at[block, band_of(which)]
        arrived(ref, wo_recv.at[block, to_band(which)])

    def wo_across(k, which):
        return wo_send_copy(col, which, (me, same_core(k)), k)

    def wo_aside(k, which):
        block = col if k == 0 else same_core(k)
        return wo_send_copy(block, which, (me, sibling), 0 if k == 0 else places + k - 1)

    def wo_partner(k):
        return wo_send_copy(same_core(k), 0, (me + 1 - 2 * odd, col), 2 * places - 2 + k)

    for part in range(PARTS):
        for kind in range(places):
            token_copy(kind, part).start()

    lane = lax.broadcasted_iota(jnp.int32, (half, width), 1)

    def turn(value):
        return pltpu.roll(value, half, 1)

    def head_at(step):
        base = lax.rem(my_head + step // 2 * 2, heads)
        return base + lax.rem(step, 2) * (1 - 2 * lax.rem(base, 2))

    def kv_copy(step, share, strip):
        head = head_at(step)
        return pltpu.make_async_remote_copy(
            src_ref=kv_own.at[head, share, strip], dst_ref=kv_all.at[me, share, strip],
            send_sem=kv_send.at[step, share, strip], recv_sem=kv_recv.at[me, share, strip],
            device_id=(head * share_count + my_share, col), device_id_type=MESH,
        )

    def forward(turn_of, step, share, strip):
        block = turn_of * share_count + my_share
        peer = my_head * share_count + lax.rem(my_share + step, share_count)
        return pltpu.make_async_remote_copy(
            src_ref=kv_all.at[block, share, strip], dst_ref=kv_all.at[block, share, strip],
            send_sem=pass_send.at[turn_of, step, share, strip],
            recv_sem=kv_recv.at[block, share, strip],
            device_id=(peer, col), device_id_type=MESH,
        )

    def relay_one(block, share, strip):
        arrived(kv_all.at[block, share, strip], kv_recv.at[block, share, strip])
        for step in range(1, share_count):
            forward(block // share_count, step, share, strip).start()

    def relay(block, strip):
        if early:
            relay_one(block, 1 - own_group, strip)
        else:
            for share in range(halves):
                relay_one(block, share, strip)

    def share_of(unit):
        place_in = lax.rem(unit, share_count)
        return jnp.where(
            lax.rem(unit // share_count, 2) == 0, place_in, share_count - 1 - place_in
        )

    def q_copy(step, share, strip):
        head = head_at(step)
        unit = me * halves + share
        return pltpu.make_async_remote_copy(
            src_ref=q_own.at[head, share, strip], dst_ref=q_all.at[unit // share_count, strip],
            send_sem=q_send.at[step, share, strip],
            recv_sem=q_recv.at[unit // share_count, strip],
            device_id=(head * share_count + share_of(unit), col), device_id_type=MESH,
        )

    def keeps_q(share):
        return share_of(me * halves + share) == my_share

    def project(group, strip):
        blocks, parts = pl.ds(group * pieces, pieces), pl.ds(strip * PARTS // 2, PARTS // 2)
        x = tok[blocks, parts].reshape(UNIT // 2, tok.shape[3])
        across = (((1,), (1,)), ((), ()))
        scale = LOG2E * half ** (-0.5)
        kf = jnp.dot(x, wqkv[1], preferred_element_type=jnp.float32)
        vt = lax.dot_general(wqv_t[1], x, across, preferred_element_type=jnp.float32)
        qt = lax.dot_general(wqv_t[0], x, across, preferred_element_type=jnp.float32) * scale
        vt, qt = vt.astype(jnp.bfloat16), qt.astype(jnp.bfloat16)
        for pair in range(heads // 2):
            cols = slice(pair * width, (pair + 1) * width)
            top, low = kf[:half, cols], kf[half:, cols]
            kv_own[2 * pair, group, strip, :half] = jnp.where(lane < half, top, turn(low)).astype(
                jnp.bfloat16
            )
            kv_own[2 * pair + 1, group, strip, :half] = jnp.where(
                lane < half, turn(top), low
            ).astype(jnp.bfloat16)
        for head in range(heads):
            rows = slice(head * half, (head + 1) * half)
            kv_own[head, group, strip, half:] = vt[rows]
            q_own[head, group, strip] = qt[rows]
        kv_all[me, group, strip] = kv_own[my_head, group, strip]
        for step in range(1, share_count):
            forward(my_head, step, group, strip).start()
        for first in range(0, heads, 2):
            for step in range(max(first, 1), first + 2):
                kv_copy(step, group, strip).start()
            for step in range(first, first + 2):
                if step > 0:
                    q_copy(step, group, strip).start()
                else:
                    stays = keeps_q(group)

                    @pl.when(stays)
                    def _():
                        q_all[(me * halves + group) // share_count, strip] = q_own[
                            my_head, group, strip
                        ]

                    @pl.when(jnp.logical_not(stays))
                    def _():
                        q_copy(0, group, strip).start()

    for copy in loads:
        copy.wait()
    for which in (0, 2):
        for k in range(1, places):
            wo_across(k, which).start()
    wqv_t[0] = wqkv[0].T
    wqv_t[1] = wqkv[2].T
    def pass_tokens(parts):
        for part in parts:
            for k in range(1, places):
                block = same_core(k)
                arrived(tok.at[block, part], tok_recv.at[block, part])
                token_copy(places + k - 1, part).start()

    def expect_tokens(parts):
        for part in parts:
            for k in range(1, places):
                block = lax.rem(place + k, places) * 2 + 1 - core
                arrived(tok.at[block, part], tok_recv.at[block, part])

    def expect_sibling():
        for part in range(PARTS):
            arrived(tok.at[sibling, part], tok_recv.at[sibling, part])

    if early:
        expect_sibling()
        for strip in range(2):
            project(own_group, strip)
        for strip in range(2):
            parts = range(strip * PARTS // 2, (strip + 1) * PARTS // 2)
            if strip == 1:
                pass_tokens(parts[:-1])
                for turn_of in range(heads):

                    @pl.when(turn_of != my_head)
                    def _():
                        for inner in range(2):
                            relay_one(turn_of * share_count + my_share, own_group, inner)

                pass_tokens(parts[-1:])
            else:
                pass_tokens(parts)
            expect_tokens(parts)
            project(1 - own_group, strip)
    else:
        pass_tokens(range(PARTS))
        expect_sibling()
        expect_tokens(range(PARTS))

        def project_next(group, carry):
            for strip in range(2):
                project(group, strip)
            return carry

        lax.fori_loop(0, halves, project_next, 0)

    for which in range(3):
        wo_aside(0, which).start()

    def unit_of(visit):
        place_in = jnp.where(lax.rem(visit, 2) == 0, my_share, share_count - 1 - my_share)
        return visit * share_count + place_in

    def score(visit, seg, kinds):
        for index in range(2):
            for side in range(2):
                keys = kv_all[seg, 1 - index, :, :half].reshape(width, width)
                both = jnp.dot(keys, q_rhs[visit, side], preferred_element_type=jnp.float32)
                for strip in range(2):
                    rows = slice(strip * width + side * half, strip * width + side * half + half)
                    s = both[strip * half : (strip + 1) * half]
                    z = jnp.minimum(s + table[kinds[index], rows], LOG_MAX)
                    lose = jnp.log(1.0 + jnp.exp2(z)) * LOG2E
                    log_take[index, rows] = z - lose
                    lose_low[index, rows] = lose.astype(jnp.bfloat16)

    def weigh():
        for index in range(2):
            tail = jnp.dot(tri[...], lose_low[index], preferred_element_type=jnp.float32)
            weight_low[index] = jnp.exp2(log_take[index] - tail).astype(jnp.bfloat16)
            later_ref[index : index + 1] = tail[0:1] + lose_low[index, 0:1].astype(jnp.float32)

    def gather(visit, seg):
        first = seg == unit_of(visit) // halves
        acc = jnp.where(first, 0.0, acc_ref[visit])
        later = jnp.where(first, 0.0, done_ref[visit, 0:1])
        for index in range(2):
            values = kv_all[seg, 1 - index, :, half:]
            values = jnp.concatenate([values[0], values[1]], axis=1)
            out = jnp.dot(values, weight_low[index], preferred_element_type=jnp.float32)
            acc = acc + jnp.exp2(-later) * out
            later = later + later_ref[index : index + 1]
        acc_ref[visit] = acc
        done_ref[visit, 0:1] = later

    def is_here(visit, index):
        unit = unit_of(visit)
        owner = lax.rem(unit, halves) * pieces + index
        return jnp.logical_and(unit // halves == me, owner == col)

    def back(visit, index):
        unit = unit_of(visit)
        owner = lax.rem(unit, halves) * pieces + index
        slot = col * heads + my_head
        return pltpu.make_async_remote_copy(
            src_ref=packed.at[visit, index], dst_ref=att.at[slot],
            send_sem=back_send.at[visit, index], recv_sem=back_recv.at[slot],
            device_id=(unit // halves, owner), device_id_type=MESH,
        )

    def send_home(visit):
        for index in range(pieces):
            top, low = acc_ref[visit, :, :width], acc_ref[visit, :, width:]
            top = pltpu.roll(top, (width - index * run) % width, 1)
            low = pltpu.roll(low, (width + run - index * run) % width, 1)
            piece = jnp.where(lane < run, top, low)[:, :device_rows]
            packed[visit, index] = piece.astype(jnp.bfloat16)
            here = is_here(visit, index)

            @pl.when(here)
            def _():
                att[col * heads + my_head] = packed[visit, index]

            @pl.when(jnp.logical_not(here))
            def _():
                back(visit, index).start()

    def relayed(block):
        return jnp.logical_and(lax.rem(block, share_count) == my_share, block != me)

    halved = blocks_per_visit == 1 and n_sp % 4 == 0
    near, quarter = n_sp // 2, n_sp // 4
    upper = my_head >= heads // 2

    def pick(low, high):
        return jnp.where(upper, high, low) if halved else low

    swept = lax.rem(my_head, 2) == 1

    def block_at(turn_count):
        distant = turn_count - near - quarter
        far = pick(turn_count, jnp.where(distant < 0, n_sp - 1 - turn_count, distant))
        close = jnp.where(swept, near - 1 - turn_count, turn_count) + pick(0, near)
        return jnp.where(turn_count < near, close, far)

    def relay_from(first, last):
        def one(index, carry):
            span = last - first
            block = block_at(first + lax.rem(index, span))

            @pl.when(relayed(block))
            def _():
                relay(block, index // span)

            return carry

        lax.fori_loop(0, 2 * (last - first), one, 0)

    def expect(block):
        @pl.when(lax.rem(block, share_count) != my_share)
        def _():
            for share in range(halves):
                for strip in range(2):
                    arrived(kv_all.at[block, share, strip], kv_recv.at[block, share, strip])

    def expect_queries(visit):
        @pl.when(unit_of(visit) // halves != me)
        def _():
            for strip in range(2):
                arrived(q_all.at[visit, strip], q_recv.at[visit, strip])

        pair = q_all[visit]
        queries = jnp.concatenate([pair[0], pair[1]], axis=1)
        q_rhs[visit, 0, :half] = queries
        q_rhs[visit, 1, half:] = queries

    turns = n_sp + near if halved else visits
    relay_from(0, near if halved else n_sp)

    def take_turn(turn_count, carry):
        if halved:

            @pl.when(turn_count == FAR_RELAY)
            def _():
                relay_from(near, near + quarter)

            @pl.when(turn_count == LAST_RELAY)
            def _():
                relay_from(near + quarter, n_sp)

            @pl.when(turn_count < n_sp)
            def _():
                expect(block_at(turn_count))

            distant = turn_count - near - quarter
            home = turn_count < near
            block = block_at(turn_count)
            late = jnp.logical_and(distant >= 0, distant < near)
            asks = jnp.logical_or(home, pick(turn_count < n_sp, late))
            asked = jnp.where(home, block, pick(turn_count, distant))

            @pl.when(asks)
            def _():
                expect_queries(asked)

            along = jnp.where(home, swept, jnp.logical_and(upper, jnp.logical_not(late)))
            rest = jnp.where(distant < 0, n_sp - 1 - turn_count, turns - 1 - turn_count)
            far_seg = jnp.where(along, rest, asked)
            seg = jnp.where(home, block, far_seg)
            visit = jnp.where(home, block, jnp.where(along, near, asked))
            far_count = pick(
                jnp.where(turn_count < n_sp, turn_count + 1, 0),
                jnp.where(late, distant + 1, near),
            )
            count = jnp.where(home, turn_count + 1, far_count)
            forth = jnp.where(along, 1, 0)
            wo_first, wo_last = near + WO_TURN, pick(n_sp - 1, n_sp + 2)
        else:
            for offset in range(blocks_per_visit):
                expect(turn_count * blocks_per_visit + offset)
            expect_queries(turn_count)
            visit, seg = turn_count, unit_of(turn_count) // halves
            count, forth = seg + 1, 0
            wo_first, wo_last = visits // 2, visits - 1

        @pl.when(turn_count == wo_first)
        def _():
            for k in range(1, places):
                wo_arrived(same_core(k), 0)
                wo_partner(k).start()
                wo_aside(k, 0).start()

        @pl.when(turn_count == wo_last)
        def _():
            for k in range(1, places):
                for which in (2, 1):
                    wo_arrived(same_core(k), which)
                    wo_aside(k, which).start()

        def step_segment(step, state):
            last_visit, last_seg, real = state
            now = visit + forth * step
            part = seg - (1 - forth) * step
            unit = unit_of(now)
            own, side = part == unit // halves, lax.rem(unit, halves)
            kinds = (jnp.where(own, 2 - side, 0), jnp.where(own, 1 - side, 0))
            weigh()
            score(now, part, kinds)
            gather(last_visit, last_seg)

            @pl.when(jnp.logical_and(last_seg == 0, real == 1))
            def _():
                send_home(last_visit)

            return now, part, jnp.int32(1)

        return lax.fori_loop(0, count, step_segment, carry)

    start = jnp.int32(0) + (block_at(0) if halved else 0)
    last_visit, last_seg, _ = lax.fori_loop(0, turns, take_turn, (start, start, jnp.int32(0)))
    weigh()
    gather(last_visit, last_seg)
    send_home(last_visit)

    my_unit = me * halves + col * device_rows // UNIT
    for source_col in range(n_tp):
        for head in range(heads):
            slot = source_col * heads + head
            source = head * share_count + share_of(my_unit)

            @pl.when(jnp.logical_not(jnp.logical_and(source == me, source_col == col)))
            def _():
                arrived(att.at[slot], back_recv.at[slot])

    att_rows[...] = att[...].reshape(att_rows.shape[1], device_rows).T
    for k in range(places):
        for which in range(3):
            wo_arrived(lax.rem(place + k, places) * 2 + 1 - core, which)
    for first in range(0, out_ref.shape[1], COLS):
        w = wfull[:, :, first : first + COLS].reshape(att_rows.shape[1], COLS)
        out_ref[:, first : first + COLS] = jnp.dot(
            att_rows[...], w, preferred_element_type=jnp.float32
        ).astype(jnp.bfloat16)

    for k in range(places):
        for which in range(3):
            wo_aside(k, which).wait_send()
    for k in range(1, places):
        wo_partner(k).wait_send()
        for which in (0, 2):
            wo_across(k, which).wait_send()
    for kind in range(2 * places - 1):
        for part in range(PARTS):
            token_copy(kind, part).wait_send()
    for share in range(halves):
        for strip in range(2):

            @pl.when(jnp.logical_not(keeps_q(share)))
            def _():
                q_copy(0, share, strip).wait_send()

            for step in range(1, heads):
                q_copy(step, share, strip).wait_send()
                kv_copy(step, share, strip).wait_send()
            for turn_of in range(heads):
                for step in range(1, share_count):
                    forward(turn_of, step, share, strip).wait_send()

    def drain(visit, carry):
        for index in range(pieces):

            @pl.when(jnp.logical_not(is_here(visit, index)))
            def _():
                back(visit, index).wait_send()

        return carry

    lax.fori_loop(0, visits, drain, 0)


def shards(tokens, w_query, w_key, w_value, head_bias, w_out):
    model, local_width = w_query.shape
    heads = head_bias.shape[0]
    half = local_width // heads
    width = 2 * half
    n_sp = lax.axis_size("sp")
    n_tp = lax.axis_size("tp")
    device_rows = tokens.shape[0]
    share_count = n_sp // heads
    halves = device_rows * n_tp // UNIT
    pieces = UNIT // device_rows
    visits = n_sp * halves // share_count
    slots = n_tp * heads
    out_width = w_out.shape[1]
    places = n_tp // 2
    kinds = 2 * places - 1

    smem = pl.BlockSpec(memory_space=pltpu.SMEM)
    anywhere = pl.BlockSpec(memory_space=pl.ANY)
    dma = pltpu.SemaphoreType.DMA

    def vmem(*shape):
        return pltpu.VMEM(shape, jnp.bfloat16)

    def wide(*shape):
        return pltpu.VMEM(shape, jnp.float32)

    return pl.pallas_call(
        functools.partial(layer_kernel, n_sp, n_tp, heads),
        out_shape=jax.ShapeDtypeStruct((device_rows, out_width), jnp.bfloat16),
        in_specs=[smem] + [anywhere] * 5,
        out_specs=pl.BlockSpec(memory_space=pltpu.VMEM),
        scratch_shapes=[
            vmem(n_tp, PARTS, device_rows // PARTS, model),
            vmem(3, model, local_width),
            vmem(2, local_width, model),
            vmem(n_tp, local_width, out_width),
            vmem(heads, halves, 2, width, width),
            vmem(heads, halves, 2, half, width),
            vmem(visits, 2, half, width),
            vmem(n_sp, halves, 2, width, width),
            vmem(visits, pieces, half, device_rows),
            vmem(slots, half, device_rows),
            vmem(device_rows, n_tp * local_width),
            vmem(UNIT, UNIT),
            wide(3, UNIT, UNIT),
            vmem(visits, 2, width, UNIT),
            wide(2, UNIT, UNIT),
            vmem(2, UNIT, UNIT),
            vmem(2, UNIT, UNIT),
            wide(visits, half, UNIT),
            wide(8, UNIT),
            wide(visits, 8, UNIT),
            dma((5,)),
            dma((kinds, PARTS)),
            dma((n_tp, PARTS)),
            dma((3 * places - 2, 3)),
            dma((n_tp, 3)),
            dma((heads, halves, 2)),
            dma((heads, share_count, halves, 2)),
            dma((n_sp, halves, 2)),
            dma((heads, halves, 2)),
            dma((visits, 2)),
            dma((visits, pieces)),
            dma((slots,)),
        ],
        compiler_params=pltpu.CompilerParams(
            collective_id=0, has_side_effects=True, vmem_limit_bytes=53 * 2**20
        ),
        name="layer",
    )(
        head_bias,
        tokens.reshape(PARTS, device_rows // PARTS, model),
        w_query, w_key, w_value, w_out,
    )


def solution(mesh):
    placed = (
        P(("sp", "tp"), None),
        P(None, "tp"),
        P(None, "tp"),
        P(None, "tp"),
        P("tp"),
        P("tp", None),
    )
    return jax.shard_map(
        shards, mesh=mesh, in_specs=placed, out_specs=P(("sp", "tp"), None), check_vma=False
    )
```

```python
import functools
import math

import jax
import jax.numpy as jnp
from jax import lax
from jax.experimental import pallas as pl
from jax.experimental.pallas import tpu as pltpu
from jax.sharding import PartitionSpec as P

MESH = pl.DeviceIdType.MESH
LOG2E = math.log2(math.e)
UNIT = 256
PARTS = 4
COLS = 512
WO_TURN = 0
FAR_RELAY = 2
LAST_RELAY = 3
LOG_MAX = 126.0
DEAD = -1e30


def layer_kernel(
    n_sp, n_tp, heads, bias_ref, tokens_ref, wq_ref, wk_ref, wv_ref, wo_ref, out_ref,
    tok, wqkv, wqv_t, wfull, kv_own, q_own, q_all, kv_all, packed, att, att_rows, tri,
    table, q_rhs, log_take, lose_low, weight_low, acc_ref, later_ref, done_ref,
    load_sem, tok_send, tok_recv, wo_send, wo_recv, kv_send, pass_send, kv_recv, q_send, q_recv,
    back_send, back_recv,
):
    me = lax.axis_index("sp")
    col = lax.axis_index("tp")
    share_count = n_sp // heads
    device_rows = PARTS * tokens_ref.shape[1]
    width = kv_own.shape[4]
    half = width // 2
    local_width = heads * half
    halves = device_rows * n_tp // UNIT
    pieces = UNIT // device_rows
    visits = n_sp * halves // share_count
    blocks_per_visit = share_count // halves
    my_head = me // share_count
    my_share = lax.rem(me, share_count)
    own_group = col // pieces
    early = pieces == 2 and halves == 2
    core = lax.rem(col, 2)
    place = col // 2
    places = n_tp // 2
    sibling = place * 2 + 1 - core

    loads = [
        pltpu.make_async_copy(src, dst, load_sem.at[index])
        for index, (src, dst) in enumerate(
            [
                (tokens_ref, tok.at[col]),
                (wq_ref, wqkv.at[0]),
                (wk_ref, wqkv.at[1]),
                (wv_ref, wqkv.at[2]),
                (wo_ref, wfull.at[col]),
            ]
        )
    ]
    for copy in loads:
        copy.start()

    barrier = pltpu.get_barrier_semaphore()
    total = n_sp * n_tp
    flat = me * n_tp + col

    def greet(step, carry):
        other = lax.rem(flat + step, total)
        pl.semaphore_signal(
            barrier, inc=1, device_id=(other // n_tp, lax.rem(other, n_tp)), device_id_type=MESH
        )
        return carry

    lax.fori_loop(1, total, greet, 0)
    bias = bias_ref[my_head] * LOG2E
    row_id = lax.broadcasted_iota(jnp.int32, (UNIT, UNIT), 0)
    col_id = lax.broadcasted_iota(jnp.int32, (UNIT, UNIT), 1)
    run = device_rows // 2
    run_bits = run.bit_length() - 1

    def position(index):
        inner = index & (width - 1)
        block = lax.shift_right_logical(inner, run_bits)
        side = lax.shift_right_logical(index, width.bit_length() - 1)
        return block * device_rows + side * run + (inner & (run - 1))

    row_id, col_id = position(row_id), position(col_id)
    tri[...] = jnp.where(col_id > row_id, 1.0, 0.0).astype(jnp.bfloat16)
    table[0] = jnp.full((UNIT, UNIT), bias, jnp.float32)
    table[1] = jnp.where(row_id < col_id, bias, DEAD)
    table[2] = jnp.full((UNIT, UNIT), DEAD, jnp.float32)
    for ref in (q_rhs, log_take, lose_low, weight_low, acc_ref, later_ref, done_ref):
        ref[...] = jnp.zeros(ref.shape, ref.dtype)
    pl.semaphore_wait(barrier, total - 1)

    def same_core(k):
        return lax.rem(place + k, places) * 2 + core

    def arrived(ref, sem):
        pltpu.make_async_copy(ref, ref, sem).wait()

    def token_copy(kind, part):
        if kind < places:
            src, block = tokens_ref.at[part], col
            target = sibling if kind == 0 else same_core(kind)
        else:
            block = same_core(kind - places + 1)
            src, target = tok.at[block, part], sibling
        return pltpu.make_async_remote_copy(
            src_ref=src, dst_ref=tok.at[block, part],
            send_sem=tok_send.at[kind, part], recv_sem=tok_recv.at[block, part],
            device_id=(me, target), device_id_type=MESH,
        )

    shared = local_width * 3 // 16
    odd = lax.rem(me, 2)

    def band_of(which):
        if which == 2:
            return pl.ds(2 * shared, local_width - 2 * shared)
        return pl.ds(pl.multiple_of((odd if which == 0 else 1 - odd) * shared, 16), shared)

    def to_band(which):
        if which == 2:
            return 2
        return odd if which == 0 else 1 - odd

    def wo_send_copy(block, which, target, slot):
        rows = band_of(which)
        return pltpu.make_async_remote_copy(
            src_ref=wfull.at[block, rows], dst_ref=wfull.at[block, rows],
            send_sem=wo_send.at[slot, which], recv_sem=wo_recv.at[block, to_band(which)],
            device_id=target, device_id_type=MESH,
        )

    def wo_arrived(block, which):
        ref = wfull.at[block, band_of(which)]
        arrived(ref, wo_recv.at[block, to_band(which)])

    def wo_across(k, which):
        return wo_send_copy(col, which, (me, same_core(k)), k)

    def wo_aside(k, which):
        block = col if k == 0 else same_core(k)
        return wo_send_copy(block, which, (me, sibling), 0 if k == 0 else places + k - 1)

    def wo_partner(k):
        return wo_send_copy(same_core(k), 0, (me + 1 - 2 * odd, col), 2 * places - 2 + k)

    for part in range(PARTS):
        for kind in range(places):
            token_copy(kind, part).start()

    lane = lax.broadcasted_iota(jnp.int32, (half, width), 1)

    def turn(value):
        return pltpu.roll(value, half, 1)

    def head_at(step):
        base = lax.rem(my_head + step // 2 * 2, heads)
        return base + lax.rem(step, 2) * (1 - 2 * lax.rem(base, 2))

    def kv_copy(step, share, strip):
        head = head_at(step)
        return pltpu.make_async_remote_copy(
            src_ref=kv_own.at[head, share, strip], dst_ref=kv_all.at[me, share, strip],
            send_sem=kv_send.at[step, share, strip], recv_sem=kv_recv.at[me, share, strip],
            device_id=(head * share_count + my_share, col), device_id_type=MESH,
        )

    def forward(turn_of, step, share, strip):
        block = turn_of * share_count + my_share
        peer = my_head * share_count + lax.rem(my_share + step, share_count)
        return pltpu.make_async_remote_copy(
            src_ref=kv_all.at[block, share, strip], dst_ref=kv_all.at[block, share, strip],
            send_sem=pass_send.at[turn_of, step, share, strip],
            recv_sem=kv_recv.at[block, share, strip],
            device_id=(peer, col), device_id_type=MESH,
        )

    def relay_one(block, share, strip):
        arrived(kv_all.at[block, share, strip], kv_recv.at[block, share, strip])
        for step in range(1, share_count):
            forward(block // share_count, step, share, strip).start()

    def relay(block, strip):
        if early:
            relay_one(block, 1 - own_group, strip)
        else:
            for share in range(halves):
                relay_one(block, share, strip)

    def share_of(unit):
        place_in = lax.rem(unit, share_count)
        return jnp.where(
            lax.rem(unit // share_count, 2) == 0, place_in, share_count - 1 - place_in
        )

    def q_copy(step, share, strip):
        head = head_at(step)
        unit = me * halves + share
        return pltpu.make_async_remote_copy(
            src_ref=q_own.at[head, share, strip], dst_ref=q_all.at[unit // share_count, strip],
            send_sem=q_send.at[step, share, strip],
            recv_sem=q_recv.at[unit // share_count, strip],
            device_id=(head * share_count + share_of(unit), col), device_id_type=MESH,
        )

    def keeps_q(share):
        return share_of(me * halves + share) == my_share

    def project(group, strip):
        blocks, parts = pl.ds(group * pieces, pieces), pl.ds(strip * PARTS // 2, PARTS // 2)
        x = tok[blocks, parts].reshape(UNIT // 2, tok.shape[3])
        across = (((1,), (1,)), ((), ()))
        scale = LOG2E * half ** (-0.5)
        kf = jnp.dot(x, wqkv[1], preferred_element_type=jnp.float32)
        vt = lax.dot_general(wqv_t[1], x, across, preferred_element_type=jnp.float32)
        qt = lax.dot_general(wqv_t[0], x, across, preferred_element_type=jnp.float32) * scale
        vt, qt = vt.astype(jnp.bfloat16), qt.astype(jnp.bfloat16)
        for pair in range(heads // 2):
            cols = slice(pair * width, (pair + 1) * width)
            top, low = kf[:half, cols], kf[half:, cols]
            kv_own[2 * pair, group, strip, :half] = jnp.where(lane < half, top, turn(low)).astype(
                jnp.bfloat16
            )
            kv_own[2 * pair + 1, group, strip, :half] = jnp.where(
                lane < half, turn(top), low
            ).astype(jnp.bfloat16)
        for head in range(heads):
            rows = slice(head * half, (head + 1) * half)
            kv_own[head, group, strip, half:] = vt[rows]
            q_own[head, group, strip] = qt[rows]
        kv_all[me, group, strip] = kv_own[my_head, group, strip]
        for step in range(1, share_count):
            forward(my_head, step, group, strip).start()
        for first in range(0, heads, 2):
            for step in range(max(first, 1), first + 2):
                kv_copy(step, group, strip).start()
            for step in range(first, first + 2):
                if step > 0:
                    q_copy(step, group, strip).start()
                else:
                    stays = keeps_q(group)

                    @pl.when(stays)
                    def _():
                        q_all[(me * halves + group) // share_count, strip] = q_own[
                            my_head, group, strip
                        ]

                    @pl.when(jnp.logical_not(stays))
                    def _():
                        q_copy(0, group, strip).start()

    for copy in loads:
        copy.wait()
    for which in (0, 2):
        for k in range(1, places):
            wo_across(k, which).start()
    wqv_t[0] = wqkv[0].T
    wqv_t[1] = wqkv[2].T
    def pass_tokens(parts):
        for part in parts:
            for k in range(1, places):
                block = same_core(k)
                arrived(tok.at[block, part], tok_recv.at[block, part])
                token_copy(places + k - 1, part).start()

    def expect_tokens(parts):
        for part in parts:
            for k in range(1, places):
                block = lax.rem(place + k, places) * 2 + 1 - core
                arrived(tok.at[block, part], tok_recv.at[block, part])

    def expect_sibling():
        for part in range(PARTS):
            arrived(tok.at[sibling, part], tok_recv.at[sibling, part])

    if early:
        expect_sibling()
        for strip in range(2):
            project(own_group, strip)
        for strip in range(2):
            parts = range(strip * PARTS // 2, (strip + 1) * PARTS // 2)
            if strip == 1:
                pass_tokens(parts[:-1])
                for turn_of in range(heads):

                    @pl.when(turn_of != my_head)
                    def _():
                        for inner in range(2):
                            relay_one(turn_of * share_count + my_share, own_group, inner)

                pass_tokens(parts[-1:])
            else:
                pass_tokens(parts)
            expect_tokens(parts)
            project(1 - own_group, strip)
    else:
        pass_tokens(range(PARTS))
        expect_sibling()
        expect_tokens(range(PARTS))

        def project_next(group, carry):
            for strip in range(2):
                project(group, strip)
            return carry

        lax.fori_loop(0, halves, project_next, 0)

    for which in range(3):
        wo_aside(0, which).start()

    def unit_of(visit):
        place_in = jnp.where(lax.rem(visit, 2) == 0, my_share, share_count - 1 - my_share)
        return visit * share_count + place_in

    def score(visit, seg, kinds):
        for index in range(2):
            for side in range(2):
                keys = kv_all[seg, 1 - index, :, :half].reshape(width, width)
                both = jnp.dot(keys, q_rhs[visit, side], preferred_element_type=jnp.float32)
                for strip in range(2):
                    rows = slice(strip * width + side * half, strip * width + side * half + half)
                    s = both[strip * half : (strip + 1) * half]
                    z = jnp.minimum(s + table[kinds[index], rows], LOG_MAX)
                    lose = jnp.log(1.0 + jnp.exp2(z)) * LOG2E
                    log_take[index, rows] = z - lose
                    lose_low[index, rows] = lose.astype(jnp.bfloat16)

    def weigh():
        for index in range(2):
            tail = jnp.dot(tri[...], lose_low[index], preferred_element_type=jnp.float32)
            weight_low[index] = jnp.exp2(log_take[index] - tail).astype(jnp.bfloat16)
            later_ref[index : index + 1] = tail[0:1] + lose_low[index, 0:1].astype(jnp.float32)

    def gather(visit, seg):
        first = seg == unit_of(visit) // halves
        acc = jnp.where(first, 0.0, acc_ref[visit])
        later = jnp.where(first, 0.0, done_ref[visit, 0:1])
        for index in range(2):
            values = kv_all[seg, 1 - index, :, half:]
            values = jnp.concatenate([values[0], values[1]], axis=1)
            out = jnp.dot(values, weight_low[index], preferred_element_type=jnp.float32)
            acc = acc + jnp.exp2(-later) * out
            later = later + later_ref[index : index + 1]
        acc_ref[visit] = acc
        done_ref[visit, 0:1] = later

    def is_here(visit, index):
        unit = unit_of(visit)
        owner = lax.rem(unit, halves) * pieces + index
        return jnp.logical_and(unit // halves == me, owner == col)

    def back(visit, index):
        unit = unit_of(visit)
        owner = lax.rem(unit, halves) * pieces + index
        slot = col * heads + my_head
        return pltpu.make_async_remote_copy(
            src_ref=packed.at[visit, index], dst_ref=att.at[slot],
            send_sem=back_send.at[visit, index], recv_sem=back_recv.at[slot],
            device_id=(unit // halves, owner), device_id_type=MESH,
        )

    def send_home(visit):
        for index in range(pieces):
            top, low = acc_ref[visit, :, :width], acc_ref[visit, :, width:]
            top = pltpu.roll(top, (width - index * run) % width, 1)
            low = pltpu.roll(low, (width + run - index * run) % width, 1)
            piece = jnp.where(lane < run, top, low)[:, :device_rows]
            packed[visit, index] = piece.astype(jnp.bfloat16)
            here = is_here(visit, index)

            @pl.when(here)
            def _():
                att[col * heads + my_head] = packed[visit, index]

            @pl.when(jnp.logical_not(here))
            def _():
                back(visit, index).start()

    def relayed(block):
        return jnp.logical_and(lax.rem(block, share_count) == my_share, block != me)

    halved = blocks_per_visit == 1 and n_sp % 4 == 0
    near, quarter = n_sp // 2, n_sp // 4
    upper = my_head >= heads // 2

    def pick(low, high):
        return jnp.where(upper, high, low) if halved else low

    swept = lax.rem(my_head, 2) == 1

    def block_at(turn_count):
        distant = turn_count - near - quarter
        far = pick(turn_count, jnp.where(distant < 0, n_sp - 1 - turn_count, distant))
        close = jnp.where(swept, near - 1 - turn_count, turn_count) + pick(0, near)
        return jnp.where(turn_count < near, close, far)

    def relay_from(first, last):
        def one(index, carry):
            span = last - first
            block = block_at(first + lax.rem(index, span))

            @pl.when(relayed(block))
            def _():
                relay(block, index // span)

            return carry

        lax.fori_loop(0, 2 * (last - first), one, 0)

    def expect(block):
        @pl.when(lax.rem(block, share_count) != my_share)
        def _():
            for share in range(halves):
                for strip in range(2):
                    arrived(kv_all.at[block, share, strip], kv_recv.at[block, share, strip])

    def expect_queries(visit):
        @pl.when(unit_of(visit) // halves != me)
        def _():
            for strip in range(2):
                arrived(q_all.at[visit, strip], q_recv.at[visit, strip])

        pair = q_all[visit]
        queries = jnp.concatenate([pair[0], pair[1]], axis=1)
        q_rhs[visit, 0, :half] = queries
        q_rhs[visit, 1, half:] = queries

    turns = n_sp + near if halved else visits
    relay_from(0, near if halved else n_sp)

    def take_turn(turn_count, carry):
        if halved:

            @pl.when(turn_count == FAR_RELAY)
            def _():
                relay_from(near, near + quarter)

            @pl.when(turn_count == LAST_RELAY)
            def _():
                relay_from(near + quarter, n_sp)

            @pl.when(turn_count < n_sp)
            def _():
                expect(block_at(turn_count))

            distant = turn_count - near - quarter
            home = turn_count < near
            block = block_at(turn_count)
            late = jnp.logical_and(distant >= 0, distant < near)
            asks = jnp.logical_or(home, pick(turn_count < n_sp, late))
            asked = jnp.where(home, block, pick(turn_count, distant))

            @pl.when(asks)
            def _():
                expect_queries(asked)

            along = jnp.where(home, swept, jnp.logical_and(upper, jnp.logical_not(late)))
            rest = jnp.where(distant < 0, n_sp - 1 - turn_count, turns - 1 - turn_count)
            far_seg = jnp.where(along, rest, asked)
            seg = jnp.where(home, block, far_seg)
            visit = jnp.where(home, block, jnp.where(along, near, asked))
            far_count = pick(
                jnp.where(turn_count < n_sp, turn_count + 1, 0),
                jnp.where(late, distant + 1, near),
            )
            count = jnp.where(home, turn_count + 1, far_count)
            forth = jnp.where(along, 1, 0)
            wo_first, wo_last = near + WO_TURN, pick(n_sp - 1, n_sp + 2)
        else:
            for offset in range(blocks_per_visit):
                expect(turn_count * blocks_per_visit + offset)
            expect_queries(turn_count)
            visit, seg = turn_count, unit_of(turn_count) // halves
            count, forth = seg + 1, 0
            wo_first, wo_last = visits // 2, visits - 1

        @pl.when(turn_count == wo_first)
        def _():
            for k in range(1, places):
                wo_arrived(same_core(k), 0)
                wo_partner(k).start()
                wo_aside(k, 0).start()

        @pl.when(turn_count == wo_last)
        def _():
            for k in range(1, places):
                for which in (2, 1):
                    wo_arrived(same_core(k), which)
                    wo_aside(k, which).start()

        def step_segment(step, state):
            last_visit, last_seg, real = state
            now = visit + forth * step
            part = seg - (1 - forth) * step
            unit = unit_of(now)
            own, side = part == unit // halves, lax.rem(unit, halves)
            kinds = (jnp.where(own, 2 - side, 0), jnp.where(own, 1 - side, 0))
            weigh()
            score(now, part, kinds)
            gather(last_visit, last_seg)

            @pl.when(jnp.logical_and(last_seg == 0, real == 1))
            def _():
                send_home(last_visit)

            return now, part, jnp.int32(1)

        return lax.fori_loop(0, count, step_segment, carry)

    start = jnp.int32(0) + (block_at(0) if halved else 0)
    last_visit, last_seg, _ = lax.fori_loop(0, turns, take_turn, (start, start, jnp.int32(0)))
    weigh()
    gather(last_visit, last_seg)
    send_home(last_visit)

    my_unit = me * halves + col * device_rows // UNIT
    for source_col in range(n_tp):
        for head in range(heads):
            slot = source_col * heads + head
            source = head * share_count + share_of(my_unit)

            @pl.when(jnp.logical_not(jnp.logical_and(source == me, source_col == col)))
            def _():
                arrived(att.at[slot], back_recv.at[slot])

    att_rows[...] = att[...].reshape(att_rows.shape[1], device_rows).T
    for k in range(places):
        for which in range(3):
            wo_arrived(lax.rem(place + k, places) * 2 + 1 - core, which)
    for first in range(0, out_ref.shape[1], COLS):
        w = wfull[:, :, first : first + COLS].reshape(att_rows.shape[1], COLS)
        out_ref[:, first : first + COLS] = jnp.dot(
            att_rows[...], w, preferred_element_type=jnp.float32
        ).astype(jnp.bfloat16)

    for k in range(places):
        for which in range(3):
            wo_aside(k, which).wait_send()
    for k in range(1, places):
        wo_partner(k).wait_send()
        for which in (0, 2):
            wo_across(k, which).wait_send()
    for kind in range(2 * places - 1):
        for part in range(PARTS):
            token_copy(kind, part).wait_send()
    for share in range(halves):
        for strip in range(2):

            @pl.when(jnp.logical_not(keeps_q(share)))
            def _():
                q_copy(0, share, strip).wait_send()

            for step in range(1, heads):
                q_copy(step, share, strip).wait_send()
                kv_copy(step, share, strip).wait_send()
            for turn_of in range(heads):
                for step in range(1, share_count):
                    forward(turn_of, step, share, strip).wait_send()

    def drain(visit, carry):
        for index in range(pieces):

            @pl.when(jnp.logical_not(is_here(visit, index)))
            def _():
                back(visit, index).wait_send()

        return carry

    lax.fori_loop(0, visits, drain, 0)


def shards(tokens, w_query, w_key, w_value, head_bias, w_out):
    model, local_width = w_query.shape
    heads = head_bias.shape[0]
    half = local_width // heads
    width = 2 * half
    n_sp = lax.axis_size("sp")
    n_tp = lax.axis_size("tp")
    device_rows = tokens.shape[0]
    share_count = n_sp // heads
    halves = device_rows * n_tp // UNIT
    pieces = UNIT // device_rows
    visits = n_sp * halves // share_count
    slots = n_tp * heads
    out_width = w_out.shape[1]
    places = n_tp // 2
    kinds = 2 * places - 1

    smem = pl.BlockSpec(memory_space=pltpu.SMEM)
    anywhere = pl.BlockSpec(memory_space=pl.ANY)
    dma = pltpu.SemaphoreType.DMA

    def vmem(*shape):
        return pltpu.VMEM(shape, jnp.bfloat16)

    def wide(*shape):
        return pltpu.VMEM(shape, jnp.float32)

    return pl.pallas_call(
        functools.partial(layer_kernel, n_sp, n_tp, heads),
        out_shape=jax.ShapeDtypeStruct((device_rows, out_width), jnp.bfloat16),
        in_specs=[smem] + [anywhere] * 5,
        out_specs=pl.BlockSpec(memory_space=pltpu.VMEM),
        scratch_shapes=[
            vmem(n_tp, PARTS, device_rows // PARTS, model),
            vmem(3, model, local_width),
            vmem(2, local_width, model),
            vmem(n_tp, local_width, out_width),
            vmem(heads, halves, 2, width, width),
            vmem(heads, halves, 2, half, width),
            vmem(visits, 2, half, width),
            vmem(n_sp, halves, 2, width, width),
            vmem(visits, pieces, half, device_rows),
            vmem(slots, half, device_rows),
            vmem(device_rows, n_tp * local_width),
            vmem(UNIT, UNIT),
            wide(3, UNIT, UNIT),
            vmem(visits, 2, width, UNIT),
            wide(2, UNIT, UNIT),
            vmem(2, UNIT, UNIT),
            vmem(2, UNIT, UNIT),
            wide(visits, half, UNIT),
            wide(8, UNIT),
            wide(visits, 8, UNIT),
            dma((5,)),
            dma((kinds, PARTS)),
            dma((n_tp, PARTS)),
            dma((3 * places - 2, 3)),
            dma((n_tp, 3)),
            dma((heads, halves, 2)),
            dma((heads, share_count, halves, 2)),
            dma((n_sp, halves, 2)),
            dma((heads, halves, 2)),
            dma((visits, 2)),
            dma((visits, pieces)),
            dma((slots,)),
        ],
        compiler_params=pltpu.CompilerParams(
            collective_id=0, has_side_effects=True, vmem_limit_bytes=53 * 2**20
        ),
        name="layer",
    )(
        head_bias,
        tokens.reshape(PARTS, device_rows // PARTS, model),
        w_query, w_key, w_value, w_out,
    )


def solution(mesh):
    placed = (
        P(("sp", "tp"), None),
        P(None, "tp"),
        P(None, "tp"),
        P(None, "tp"),
        P("tp"),
        P("tp", None),
    )
    return jax.shard_map(
        shards, mesh=mesh, in_specs=placed, out_specs=P(("sp", "tp"), None), check_vma=False
    )
```

```python
import functools
import math

import jax
import jax.numpy as jnp
from jax import lax
from jax.experimental import pallas as pl
from jax.experimental.pallas import tpu as pltpu
from jax.sharding import PartitionSpec as P

MESH = pl.DeviceIdType.MESH
LOG2E = math.log2(math.e)
UNIT = 256
PARTS = 4
COLS = 512
WO_TURN = 0
FAR_RELAY = 2
LAST_RELAY = 3
LOG_MAX = 126.0
DEAD = -1e30


def layer_kernel(
    n_sp, n_tp, heads, bias_ref, tokens_ref, wq_ref, wk_ref, wv_ref, wo_ref, out_ref,
    tok, wqkv, wqv_t, wfull, kv_own, q_own, q_all, kv_all, packed, att, att_rows, tri,
    table, q_rhs, log_take, lose_low, weight_low, acc_ref, later_ref, done_ref,
    load_sem, tok_send, tok_recv, wo_send, wo_recv, kv_send, pass_send, kv_recv, q_send, q_recv,
    back_send, back_recv,
):
    me = lax.axis_index("sp")
    col = lax.axis_index("tp")
    share_count = n_sp // heads
    device_rows = PARTS * tokens_ref.shape[1]
    width = kv_own.shape[4]
    half = width // 2
    local_width = heads * half
    halves = device_rows * n_tp // UNIT
    pieces = UNIT // device_rows
    visits = n_sp * halves // share_count
    blocks_per_visit = share_count // halves
    my_head = me // share_count
    my_share = lax.rem(me, share_count)
    own_group = col // pieces
    early = pieces == 2 and halves == 2
    core = lax.rem(col, 2)
    place = col // 2
    places = n_tp // 2
    sibling = place * 2 + 1 - core

    loads = [
        pltpu.make_async_copy(src, dst, load_sem.at[index])
        for index, (src, dst) in enumerate(
            [
                (tokens_ref, tok.at[col]),
                (wq_ref, wqkv.at[0]),
                (wk_ref, wqkv.at[1]),
                (wv_ref, wqkv.at[2]),
                (wo_ref, wfull.at[col]),
            ]
        )
    ]
    for copy in loads:
        copy.start()

    barrier = pltpu.get_barrier_semaphore()
    total = n_sp * n_tp
    flat = me * n_tp + col

    def greet(step, carry):
        other = lax.rem(flat + step, total)
        pl.semaphore_signal(
            barrier, inc=1, device_id=(other // n_tp, lax.rem(other, n_tp)), device_id_type=MESH
        )
        return carry

    lax.fori_loop(1, total, greet, 0)
    bias = bias_ref[my_head] * LOG2E
    row_id = lax.broadcasted_iota(jnp.int32, (UNIT, UNIT), 0)
    col_id = lax.broadcasted_iota(jnp.int32, (UNIT, UNIT), 1)
    run = device_rows // 2
    run_bits = run.bit_length() - 1

    def position(index):
        inner = index & (width - 1)
        block = lax.shift_right_logical(inner, run_bits)
        side = lax.shift_right_logical(index, width.bit_length() - 1)
        return block * device_rows + side * run + (inner & (run - 1))

    row_id, col_id = position(row_id), position(col_id)
    tri[...] = jnp.where(col_id > row_id, 1.0, 0.0).astype(jnp.bfloat16)
    table[0] = jnp.full((UNIT, UNIT), bias, jnp.float32)
    table[1] = jnp.where(row_id < col_id, bias, DEAD)
    table[2] = jnp.full((UNIT, UNIT), DEAD, jnp.float32)
    for ref in (q_rhs, log_take, lose_low, weight_low, acc_ref, later_ref, done_ref):
        ref[...] = jnp.zeros(ref.shape, ref.dtype)
    pl.semaphore_wait(barrier, total - 1)

    def same_core(k):
        return lax.rem(place + k, places) * 2 + core

    def arrived(ref, sem):
        pltpu.make_async_copy(ref, ref, sem).wait()

    def token_copy(kind, part):
        if kind < places:
            src, block = tokens_ref.at[part], col
            target = sibling if kind == 0 else same_core(kind)
        else:
            block = same_core(kind - places + 1)
            src, target = tok.at[block, part], sibling
        return pltpu.make_async_remote_copy(
            src_ref=src, dst_ref=tok.at[block, part],
            send_sem=tok_send.at[kind, part], recv_sem=tok_recv.at[block, part],
            device_id=(me, target), device_id_type=MESH,
        )

    shared = local_width * 3 // 16
    odd = lax.rem(me, 2)

    def band_of(which):
        if which == 2:
            return pl.ds(2 * shared, local_width - 2 * shared)
        return pl.ds(pl.multiple_of((odd if which == 0 else 1 - odd) * shared, 16), shared)

    def to_band(which):
        if which == 2:
            return 2
        return odd if which == 0 else 1 - odd

    def wo_send_copy(block, which, target, slot):
        rows = band_of(which)
        return pltpu.make_async_remote_copy(
            src_ref=wfull.at[block, rows], dst_ref=wfull.at[block, rows],
            send_sem=wo_send.at[slot, which], recv_sem=wo_recv.at[block, to_band(which)],
            device_id=target, device_id_type=MESH,
        )

    def wo_arrived(block, which):
        ref = wfull.at[block, band_of(which)]
        arrived(ref, wo_recv.at[block, to_band(which)])

    def wo_across(k, which):
        return wo_send_copy(col, which, (me, same_core(k)), k)

    def wo_aside(k, which):
        block = col if k == 0 else same_core(k)
        return wo_send_copy(block, which, (me, sibling), 0 if k == 0 else places + k - 1)

    def wo_partner(k):
        return wo_send_copy(same_core(k), 0, (me + 1 - 2 * odd, col), 2 * places - 2 + k)

    for part in range(PARTS):
        for kind in range(places):
            token_copy(kind, part).start()

    lane = lax.broadcasted_iota(jnp.int32, (half, width), 1)

    def turn(value):
        return pltpu.roll(value, half, 1)

    def head_at(step):
        base = lax.rem(my_head + step // 2 * 2, heads)
        return base + lax.rem(step, 2) * (1 - 2 * lax.rem(base, 2))

    def kv_copy(step, share, strip):
        head = head_at(step)
        return pltpu.make_async_remote_copy(
            src_ref=kv_own.at[head, share, strip], dst_ref=kv_all.at[me, share, strip],
            send_sem=kv_send.at[step, share, strip], recv_sem=kv_recv.at[me, share, strip],
            device_id=(head * share_count + my_share, col), device_id_type=MESH,
        )

    def forward(turn_of, step, share, strip):
        block = turn_of * share_count + my_share
        peer = my_head * share_count + lax.rem(my_share + step, share_count)
        return pltpu.make_async_remote_copy(
            src_ref=kv_all.at[block, share, strip], dst_ref=kv_all.at[block, share, strip],
            send_sem=pass_send.at[turn_of, step, share, strip],
            recv_sem=kv_recv.at[block, share, strip],
            device_id=(peer, col), device_id_type=MESH,
        )

    def relay_one(block, share, strip):
        arrived(kv_all.at[block, share, strip], kv_recv.at[block, share, strip])
        for step in range(1, share_count):
            forward(block // share_count, step, share, strip).start()

    def relay(block, strip):
        if early:
            relay_one(block, 1 - own_group, strip)
        else:
            for share in range(halves):
                relay_one(block, share, strip)

    def share_of(unit):
        place_in = lax.rem(unit, share_count)
        return jnp.where(
            lax.rem(unit // share_count, 2) == 0, place_in, share_count - 1 - place_in
        )

    def q_copy(step, share, strip):
        head = head_at(step)
        unit = me * halves + share
        return pltpu.make_async_remote_copy(
            src_ref=q_own.at[head, share, strip], dst_ref=q_all.at[unit // share_count, strip],
            send_sem=q_send.at[step, share, strip],
            recv_sem=q_recv.at[unit // share_count, strip],
            device_id=(head * share_count + share_of(unit), col), device_id_type=MESH,
        )

    def keeps_q(share):
        return share_of(me * halves + share) == my_share

    def project(group, strip):
        blocks, parts = pl.ds(group * pieces, pieces), pl.ds(strip * PARTS // 2, PARTS // 2)
        x = tok[blocks, parts].reshape(UNIT // 2, tok.shape[3])
        across = (((1,), (1,)), ((), ()))
        scale = LOG2E * half ** (-0.5)
        kf = jnp.dot(x, wqkv[1], preferred_element_type=jnp.float32)
        vt = lax.dot_general(wqv_t[1], x, across, preferred_element_type=jnp.float32)
        qt = lax.dot_general(wqv_t[0], x, across, preferred_element_type=jnp.float32) * scale
        vt, qt = vt.astype(jnp.bfloat16), qt.astype(jnp.bfloat16)
        for pair in range(heads // 2):
            cols = slice(pair * width, (pair + 1) * width)
            top, low = kf[:half, cols], kf[half:, cols]
            kv_own[2 * pair, group, strip, :half] = jnp.where(lane < half, top, turn(low)).astype(
                jnp.bfloat16
            )
            kv_own[2 * pair + 1, group, strip, :half] = jnp.where(
                lane < half, turn(top), low
            ).astype(jnp.bfloat16)
        for head in range(heads):
            rows = slice(head * half, (head + 1) * half)
            kv_own[head, group, strip, half:] = vt[rows]
            q_own[head, group, strip] = qt[rows]
        kv_all[me, group, strip] = kv_own[my_head, group, strip]
        for step in range(1, share_count):
            forward(my_head, step, group, strip).start()
        for first in range(0, heads, 2):
            for step in range(max(first, 1), first + 2):
                kv_copy(step, group, strip).start()
            for step in range(first, first + 2):
                if step > 0:
                    q_copy(step, group, strip).start()
                else:
                    stays = keeps_q(group)

                    @pl.when(stays)
                    def _():
                        q_all[(me * halves + group) // share_count, strip] = q_own[
                            my_head, group, strip
                        ]

                    @pl.when(jnp.logical_not(stays))
                    def _():
                        q_copy(0, group, strip).start()

    for copy in loads:
        copy.wait()
    for which in (0, 2):
        for k in range(1, places):
            wo_across(k, which).start()
    wqv_t[0] = wqkv[0].T
    wqv_t[1] = wqkv[2].T
    def pass_tokens(parts):
        for part in parts:
            for k in range(1, places):
                block = same_core(k)
                arrived(tok.at[block, part], tok_recv.at[block, part])
                token_copy(places + k - 1, part).start()

    def expect_tokens(parts):
        for part in parts:
            for k in range(1, places):
                block = lax.rem(place + k, places) * 2 + 1 - core
                arrived(tok.at[block, part], tok_recv.at[block, part])

    def expect_sibling():
        for part in range(PARTS):
            arrived(tok.at[sibling, part], tok_recv.at[sibling, part])

    if early:
        expect_sibling()
        for strip in range(2):
            project(own_group, strip)
        for strip in range(2):
            parts = range(strip * PARTS // 2, (strip + 1) * PARTS // 2)
            if strip == 1:
                pass_tokens(parts[:-1])
                for turn_of in range(heads):

                    @pl.when(turn_of != my_head)
                    def _():
                        for inner in range(2):
                            relay_one(turn_of * share_count + my_share, own_group, inner)

                pass_tokens(parts[-1:])
            else:
                pass_tokens(parts)
            expect_tokens(parts)
            project(1 - own_group, strip)
    else:
        pass_tokens(range(PARTS))
        expect_sibling()
        expect_tokens(range(PARTS))

        def project_next(group, carry):
            for strip in range(2):
                project(group, strip)
            return carry

        lax.fori_loop(0, halves, project_next, 0)

    for which in range(3):
        wo_aside(0, which).start()

    def unit_of(visit):
        place_in = jnp.where(lax.rem(visit, 2) == 0, my_share, share_count - 1 - my_share)
        return visit * share_count + place_in

    def score(visit, seg, kinds):
        for index in range(2):
            for side in range(2):
                keys = kv_all[seg, 1 - index, :, :half].reshape(width, width)
                both = jnp.dot(keys, q_rhs[visit, side], preferred_element_type=jnp.float32)
                for strip in range(2):
                    rows = slice(strip * width + side * half, strip * width + side * half + half)
                    s = both[strip * half : (strip + 1) * half]
                    z = jnp.minimum(s + table[kinds[index], rows], LOG_MAX)
                    lose = jnp.log(1.0 + jnp.exp2(z)) * LOG2E
                    log_take[index, rows] = z - lose
                    lose_low[index, rows] = lose.astype(jnp.bfloat16)

    def weigh():
        for index in range(2):
            tail = jnp.dot(tri[...], lose_low[index], preferred_element_type=jnp.float32)
            weight_low[index] = jnp.exp2(log_take[index] - tail).astype(jnp.bfloat16)
            later_ref[index : index + 1] = tail[0:1] + lose_low[index, 0:1].astype(jnp.float32)

    def gather(visit, seg):
        first = seg == unit_of(visit) // halves
        acc = jnp.where(first, 0.0, acc_ref[visit])
        later = jnp.where(first, 0.0, done_ref[visit, 0:1])
        for index in range(2):
            values = kv_all[seg, 1 - index, :, half:]
            values = jnp.concatenate([values[0], values[1]], axis=1)
            out = jnp.dot(values, weight_low[index], preferred_element_type=jnp.float32)
            acc = acc + jnp.exp2(-later) * out
            later = later + later_ref[index : index + 1]
        acc_ref[visit] = acc
        done_ref[visit, 0:1] = later

    def is_here(visit, index):
        unit = unit_of(visit)
        owner = lax.rem(unit, halves) * pieces + index
        return jnp.logical_and(unit // halves == me, owner == col)

    def back(visit, index):
        unit = unit_of(visit)
        owner = lax.rem(unit, halves) * pieces + index
        slot = col * heads + my_head
        return pltpu.make_async_remote_copy(
            src_ref=packed.at[visit, index], dst_ref=att.at[slot],
            send_sem=back_send.at[visit, index], recv_sem=back_recv.at[slot],
            device_id=(unit // halves, owner), device_id_type=MESH,
        )

    def send_home(visit):
        for index in range(pieces):
            top, low = acc_ref[visit, :, :width], acc_ref[visit, :, width:]
            top = pltpu.roll(top, (width - index * run) % width, 1)
            low = pltpu.roll(low, (width + run - index * run) % width, 1)
            piece = jnp.where(lane < run, top, low)[:, :device_rows]
            packed[visit, index] = piece.astype(jnp.bfloat16)
            here = is_here(visit, index)

            @pl.when(here)
            def _():
                att[col * heads + my_head] = packed[visit, index]

            @pl.when(jnp.logical_not(here))
            def _():
                back(visit, index).start()

    def relayed(block):
        return jnp.logical_and(lax.rem(block, share_count) == my_share, block != me)

    halved = blocks_per_visit == 1 and n_sp % 4 == 0
    near, quarter = n_sp // 2, n_sp // 4
    upper = my_head >= heads // 2

    def pick(low, high):
        return jnp.where(upper, high, low) if halved else low

    swept = lax.rem(my_head, 2) == 1

    def block_at(turn_count):
        distant = turn_count - near - quarter
        far = pick(turn_count, jnp.where(distant < 0, n_sp - 1 - turn_count, distant))
        close = jnp.where(swept, near - 1 - turn_count, turn_count) + pick(0, near)
        return jnp.where(turn_count < near, close, far)

    def relay_from(first, last):
        def one(index, carry):
            span = last - first
            block = block_at(first + lax.rem(index, span))

            @pl.when(relayed(block))
            def _():
                relay(block, index // span)

            return carry

        lax.fori_loop(0, 2 * (last - first), one, 0)

    def expect(block):
        @pl.when(lax.rem(block, share_count) != my_share)
        def _():
            for share in range(halves):
                for strip in range(2):
                    arrived(kv_all.at[block, share, strip], kv_recv.at[block, share, strip])

    def expect_queries(visit):
        @pl.when(unit_of(visit) // halves != me)
        def _():
            for strip in range(2):
                arrived(q_all.at[visit, strip], q_recv.at[visit, strip])

        pair = q_all[visit]
        queries = jnp.concatenate([pair[0], pair[1]], axis=1)
        q_rhs[visit, 0, :half] = queries
        q_rhs[visit, 1, half:] = queries

    def finish_wo():
        for k in range(1, places):
            for which in (2, 1):
                wo_arrived(same_core(k), which)
                wo_aside(k, which).start()

    turns = n_sp + near if halved else visits
    relay_from(0, near if halved else n_sp)

    def take_turn(turn_count, carry):
        if halved:

            @pl.when(turn_count == FAR_RELAY)
            def _():
                relay_from(near, near + quarter)

            @pl.when(turn_count == LAST_RELAY)
            def _():
                relay_from(near + quarter, n_sp)

            @pl.when(turn_count < n_sp)
            def _():
                expect(block_at(turn_count))

            distant = turn_count - near - quarter
            home = turn_count < near
            block = block_at(turn_count)
            late = jnp.logical_and(distant >= 0, distant < near)
            asks = jnp.logical_or(home, pick(turn_count < n_sp, late))
            asked = jnp.where(home, block, pick(turn_count, distant))

            @pl.when(asks)
            def _():
                expect_queries(asked)

            along = jnp.where(home, swept, jnp.logical_and(upper, jnp.logical_not(late)))
            rest = jnp.where(distant < 0, n_sp - 1 - turn_count, turns - 1 - turn_count)
            far_seg = jnp.where(along, rest, asked)
            seg = jnp.where(home, block, far_seg)
            visit = jnp.where(home, block, jnp.where(along, near, asked))
            far_count = pick(
                jnp.where(turn_count < n_sp, turn_count + 1, 0),
                jnp.where(late, distant + 1, near),
            )
            count = jnp.where(home, turn_count + 1, far_count)
            forth = jnp.where(along, 1, 0)
            wo_first, wo_last = near + WO_TURN, pick(turns, n_sp + 2)
        else:
            for offset in range(blocks_per_visit):
                expect(turn_count * blocks_per_visit + offset)
            expect_queries(turn_count)
            visit, seg = turn_count, unit_of(turn_count) // halves
            count, forth = seg + 1, 0
            wo_first, wo_last = visits // 2, visits - 1

        @pl.when(turn_count == wo_first)
        def _():
            for k in range(1, places):
                wo_arrived(same_core(k), 0)
                wo_partner(k).start()
                wo_aside(k, 0).start()

        @pl.when(turn_count == wo_last)
        def _():
            finish_wo()

        def step_segment(step, state):
            last_visit, last_seg, real = state
            now = visit + forth * step
            part = seg - (1 - forth) * step
            unit = unit_of(now)
            own, side = part == unit // halves, lax.rem(unit, halves)
            kinds = (jnp.where(own, 2 - side, 0), jnp.where(own, 1 - side, 0))
            weigh()
            score(now, part, kinds)
            gather(last_visit, last_seg)

            @pl.when(jnp.logical_and(last_seg == 0, real == 1))
            def _():
                send_home(last_visit)

            return now, part, jnp.int32(1)

        return lax.fori_loop(0, count, step_segment, carry)

    start = jnp.int32(0) + (block_at(0) if halved else 0)
    last_visit, last_seg, _ = lax.fori_loop(0, turns, take_turn, (start, start, jnp.int32(0)))
    weigh()
    gather(last_visit, last_seg)
    send_home(last_visit)

    if halved:

        @pl.when(jnp.logical_not(upper))
        def _():
            finish_wo()

    my_unit = me * halves + col * device_rows // UNIT
    for source_col in range(n_tp):
        for head in range(heads):
            slot = source_col * heads + head
            source = head * share_count + share_of(my_unit)

            @pl.when(jnp.logical_not(jnp.logical_and(source == me, source_col == col)))
            def _():
                arrived(att.at[slot], back_recv.at[slot])

    att_rows[...] = att[...].reshape(att_rows.shape[1], device_rows).T
    for k in range(places):
        for which in range(3):
            wo_arrived(lax.rem(place + k, places) * 2 + 1 - core, which)
    for first in range(0, out_ref.shape[1], COLS):
        w = wfull[:, :, first : first + COLS].reshape(att_rows.shape[1], COLS)
        out_ref[:, first : first + COLS] = jnp.dot(
            att_rows[...], w, preferred_element_type=jnp.float32
        ).astype(jnp.bfloat16)

    for k in range(places):
        for which in range(3):
            wo_aside(k, which).wait_send()
    for k in range(1, places):
        wo_partner(k).wait_send()
        for which in (0, 2):
            wo_across(k, which).wait_send()
    for kind in range(2 * places - 1):
        for part in range(PARTS):
            token_copy(kind, part).wait_send()
    for share in range(halves):
        for strip in range(2):

            @pl.when(jnp.logical_not(keeps_q(share)))
            def _():
                q_copy(0, share, strip).wait_send()

            for step in range(1, heads):
                q_copy(step, share, strip).wait_send()
                kv_copy(step, share, strip).wait_send()
            for turn_of in range(heads):
                for step in range(1, share_count):
                    forward(turn_of, step, share, strip).wait_send()

    def drain(visit, carry):
        for index in range(pieces):

            @pl.when(jnp.logical_not(is_here(visit, index)))
            def _():
                back(visit, index).wait_send()

        return carry

    lax.fori_loop(0, visits, drain, 0)


def shards(tokens, w_query, w_key, w_value, head_bias, w_out):
    model, local_width = w_query.shape
    heads = head_bias.shape[0]
    half = local_width // heads
    width = 2 * half
    n_sp = lax.axis_size("sp")
    n_tp = lax.axis_size("tp")
    device_rows = tokens.shape[0]
    share_count = n_sp // heads
    halves = device_rows * n_tp // UNIT
    pieces = UNIT // device_rows
    visits = n_sp * halves // share_count
    slots = n_tp * heads
    out_width = w_out.shape[1]
    places = n_tp // 2
    kinds = 2 * places - 1

    smem = pl.BlockSpec(memory_space=pltpu.SMEM)
    anywhere = pl.BlockSpec(memory_space=pl.ANY)
    dma = pltpu.SemaphoreType.DMA

    def vmem(*shape):
        return pltpu.VMEM(shape, jnp.bfloat16)

    def wide(*shape):
        return pltpu.VMEM(shape, jnp.float32)

    return pl.pallas_call(
        functools.partial(layer_kernel, n_sp, n_tp, heads),
        out_shape=jax.ShapeDtypeStruct((device_rows, out_width), jnp.bfloat16),
        in_specs=[smem] + [anywhere] * 5,
        out_specs=pl.BlockSpec(memory_space=pltpu.VMEM),
        scratch_shapes=[
            vmem(n_tp, PARTS, device_rows // PARTS, model),
            vmem(3, model, local_width),
            vmem(2, local_width, model),
            vmem(n_tp, local_width, out_width),
            vmem(heads, halves, 2, width, width),
            vmem(heads, halves, 2, half, width),
            vmem(visits, 2, half, width),
            vmem(n_sp, halves, 2, width, width),
            vmem(visits, pieces, half, device_rows),
            vmem(slots, half, device_rows),
            vmem(device_rows, n_tp * local_width),
            vmem(UNIT, UNIT),
            wide(3, UNIT, UNIT),
            vmem(visits, 2, width, UNIT),
            wide(2, UNIT, UNIT),
            vmem(2, UNIT, UNIT),
            vmem(2, UNIT, UNIT),
            wide(visits, half, UNIT),
            wide(8, UNIT),
            wide(visits, 8, UNIT),
            dma((5,)),
            dma((kinds, PARTS)),
            dma((n_tp, PARTS)),
            dma((3 * places - 2, 3)),
            dma((n_tp, 3)),
            dma((heads, halves, 2)),
            dma((heads, share_count, halves, 2)),
            dma((n_sp, halves, 2)),
            dma((heads, halves, 2)),
            dma((visits, 2)),
            dma((visits, pieces)),
            dma((slots,)),
        ],
        compiler_params=pltpu.CompilerParams(
            collective_id=0, has_side_effects=True, vmem_limit_bytes=53 * 2**20
        ),
        name="layer",
    )(
        head_bias,
        tokens.reshape(PARTS, device_rows // PARTS, model),
        w_query, w_key, w_value, w_out,
    )


def solution(mesh):
    placed = (
        P(("sp", "tp"), None),
        P(None, "tp"),
        P(None, "tp"),
        P(None, "tp"),
        P("tp"),
        P("tp", None),
    )
    return jax.shard_map(
        shards, mesh=mesh, in_specs=placed, out_specs=P(("sp", "tp"), None), check_vma=False
    )
```
